32 devices in a mesh: grp: 2 (over y), sp: 4 (over z), tp: 4 (over x, core).
Axes of the slice: x: 2, y: 2, z: 4, core: 2. Of those that a mesh axis runs over, the one named last changes fastest.
Arguments:
- tokens: bfloat16 [2048, 2048], P(('grp', 'sp', 'tp')), parts along dimension 0, may hold values from -6 to 6
- norm_gain: float32 [2048], replicated, may hold values from 0.1 to 1.9
- conv_b_w: bfloat16 [2048, 1024], P('sp', 'tp'), may hold values from -0.125 to 0.125
- conv_c_w: bfloat16 [2048, 1024], P('sp', 'tp'), may hold values from -0.125 to 0.125
- conv_x_w: bfloat16 [2048, 1024], P('sp', 'tp'), may hold values from -0.125 to 0.125
- query_w: bfloat16 [2048, 1024], P('sp', 'tp'), may hold values from -1 to 1
- key_w: bfloat16 [2048, 256], P('sp', 'tp'), may hold values from -2 to 2
- value_w: bfloat16 [2048, 256], P('sp', 'tp'), may hold values from -0.125 to 0.125
- conv_taps: float32 [3, 1024], P(None, 'tp'), may hold values from -3.5 to 3.5
- gate_cache: float32 [2048, 16], P('grp', 'tp'), parts along dimension 0, as said below
- out_conv_w: bfloat16 [1024, 2048], P('tp'), may hold values from -0.1875 to 0.1875
- out_attn_w: bfloat16 [1024, 2048], P('tp'), may hold values from -0.75 to 0.75
Outputs:
- mixed: bfloat16 [2048, 2048], P(('grp', 'sp', 'tp')), parts along dimension 0
- log_total: float32 [2048, 16], P(('grp', 'sp'), 'tp'), parts along dimension 0
The draws below stay inside these ranges and needn't reach their ends.
There are 2 independent parts, one for each index of `grp`. The reference program is written for one: setup_inputs(seed, part) draws one part's arguments, and reference() takes and returns one part's arrays. A program takes and returns all parts, laid end to end along the dimension named above; an argument that names none is the same for every part. Nothing has to cross between parts.
Inputs may be any that keep to these rules, and one draw needn't show every extreme that they name: `gate_cache`: never rises along positions; starts at or below zero.
All inputs are finite; a program needn't handle non-finite values.
Results may differ from the reference program's by a relative error of at most 0.017.
The reference program's roundings to bfloat16 on the way count: a program that leaves them out, or rounds other values in their place, can miss the bound.
Values may be sent and summed in bfloat16 or wider, within the bound.
A program may use at most 64 MiB of HBM per device.

```python
import jax
import jax.numpy as jnp
from jax import lax

D = 2048
CONV = 1024
QH = 16
KVH = 4
HD = 64
CW = 3
TOK_DEV = 256
SEQUENCE_LENGTH = 1024
N_TP = 4


def query_key_pair(key):
    base = jax.random.fold_in(key, 11)
    first, second = jax.random.split(base)
    query_f = jnp.clip(jax.random.normal(first, (D, QH * HD), jnp.float32), -5.0, 5.0) * D ** (-0.5)
    noise = jnp.clip(jax.random.normal(second, (D, KVH * HD), jnp.float32), -5.0, 5.0) * D ** (-0.5)
    key_f = noise
    return (query_f, jnp.clip(key_f, -2.0, 2.0))


def draw_query_w(key, part):
    pair = query_key_pair(key)
    return pair[0].astype(jnp.bfloat16)


def draw_key_w(key, part):
    pair = query_key_pair(key)
    return pair[1].astype(jnp.bfloat16)


def draw_gate_cache(key, part):
    keys = jax.random.split(key, 7)
    order = jax.random.permutation(keys[0], QH)
    fast = order < QH // 2
    fast_rate = 1.0 / 40.0 * jnp.exp(jax.random.uniform(keys[1], (QH,), jnp.float32, -0.5, 0.5))
    slow_rate = 0.6 / SEQUENCE_LENGTH * jnp.exp(jax.random.uniform(keys[6], (QH,), jnp.float32, -0.5, 0.5))
    decay_speed = jnp.where(fast, fast_rate, slow_rate)
    blocks = SEQUENCE_LENGTH // TOK_DEV
    scale_per_block = jnp.exp(jax.random.uniform(keys[2], (blocks, QH), jnp.float32, -0.9, 0.9))
    scale_per_block = jnp.repeat(scale_per_block, TOK_DEV, axis=0)
    coarse_estimate = jnp.exp(jax.random.uniform(keys[3], (SEQUENCE_LENGTH, QH), jnp.float32, -1.0, 1.0))
    chosen_locations = jax.random.randint(keys[4], (3,), 0, SEQUENCE_LENGTH)
    spike_amplitude = jnp.zeros((SEQUENCE_LENGTH,), jnp.float32).at[chosen_locations].set(1.0)
    objective_value = jax.random.uniform(keys[5], (QH,), jnp.float32, 0.2, 0.5) * (1.0 - fast.astype(jnp.float32))
    gate_logarithm = -(decay_speed[None, :] * scale_per_block * coarse_estimate + spike_amplitude[:, None] * objective_value[None, :])
    return jnp.cumsum(gate_logarithm, axis=0)


def levels(stream_key, extent, cuts, low, largest):
    loudness, own = 1.0, jax.random.fold_in(stream_key, 6)
    for dim, parts in cuts:
        steps = jnp.exp(jax.random.uniform(jax.random.fold_in(own, dim), (parts,), jnp.float32, low / len(cuts), largest / len(cuts)))
        loudness = loudness * jnp.repeat(steps, extent[dim] // parts).reshape([-1 if axis == dim else 1 for axis in range(len(extent))])
    return loudness


def bell_draw(key, dims, deviation, most, cuts=(), held_as=jnp.bfloat16):
    gain = levels(key, dims, cuts, -0.22, 0.18) if cuts else 1.0
    values = jax.random.normal(key, dims, jnp.float32) * deviation * gain
    return jnp.minimum(jnp.maximum(values, -most), most).astype(held_as)


def setup_inputs(seed: int = 0, part: int = 0) -> dict:
    seeds = jax.random.split(jax.random.key(seed), 13)
    part_splits = jax.random.split(jax.random.fold_in(seeds[12], part), 13)
    return {
        "tokens": bell_draw(part_splits[0], (SEQUENCE_LENGTH, D), 1.0, 6.0, ((0, 16),)),
        "norm_gain": jnp.clip(1.0 + 0.18 * jax.random.normal(seeds[1], (D,), jnp.float32), 0.1, 1.9),
        "conv_b_w": bell_draw(seeds[2], (D, CONV), D ** -0.5, 0.125, ((0, 4), (1, 4))),
        "conv_c_w": bell_draw(seeds[3], (D, CONV), D ** -0.5, 0.125, ((0, 4), (1, 4))),
        "conv_x_w": bell_draw(seeds[4], (D, CONV), D ** -0.5, 0.125, ((0, 4), (1, 4))),
        "query_w": draw_query_w(jax.random.fold_in(seeds[12], 71), part),
        "key_w": draw_key_w(jax.random.fold_in(seeds[12], 71), part),
        "value_w": bell_draw(seeds[7], (D, KVH * HD), D ** -0.5, 0.125, ((0, 4), (1, 4))),
        "conv_taps": bell_draw(seeds[8], (CW, CONV), CW ** -0.5, 3.5, ((1, 4),), jnp.float32),
        "gate_cache": draw_gate_cache(jax.random.fold_in(jax.random.fold_in(seeds[12], part), 71), part),
        "out_conv_w": bell_draw(seeds[10], (CONV, D), CONV ** -0.5, 0.1875, ((0, 4),)),
        "out_attn_w": bell_draw(seeds[11], (QH * HD, D), (QH * HD // 16) ** -0.5, 0.75, ((0, 4),)),
    }


def reference(tokens, norm_gain, conv_b_w, conv_c_w, conv_x_w, query_w, key_w, value_w, conv_taps, gate_cache, out_conv_w, out_attn_w):
    xf = tokens.astype(jnp.float32)
    scale_rows = lax.rsqrt(lax.optimization_barrier(jnp.mean(xf * xf, axis=-1, keepdims=True)) + 1e-05)
    normed = (xf * norm_gain).astype(jnp.bfloat16)

    def project(weight):
        return (jnp.dot(normed, weight, preferred_element_type=jnp.float32) * scale_rows).astype(jnp.bfloat16)
    gate_b = project(conv_b_w)
    gate_c = project(conv_c_w)
    conv_in = project(conv_x_w)
    query = project(query_w)
    key = project(key_w)
    value = project(value_w)
    conv_src = (gate_c.astype(jnp.float32) * conv_in.astype(jnp.float32)).astype(jnp.bfloat16)
    padded = jnp.concatenate([jnp.zeros((CW - 1, CONV), jnp.bfloat16), conv_src], axis=0)
    filtered = jnp.zeros((SEQUENCE_LENGTH, CONV), jnp.float32)
    for tap in range(CW):
        filtered = filtered + conv_taps[tap][None, :] * padded[tap:tap + SEQUENCE_LENGTH].astype(jnp.float32)
    conv_out = (gate_b.astype(jnp.float32) * filtered).astype(jnp.bfloat16)
    group = QH // KVH
    q_block = min(256, SEQUENCE_LENGTH)
    n_blocks = SEQUENCE_LENGTH // q_block
    heads_q = query.reshape(SEQUENCE_LENGTH, KVH, group, HD)
    keys_f = key.reshape(SEQUENCE_LENGTH, KVH, HD).astype(jnp.float32)
    values_f = value.reshape(SEQUENCE_LENGTH, KVH, HD).astype(jnp.float32)
    key_gate = gate_cache.T.reshape(KVH, group, 1, SEQUENCE_LENGTH)
    key_pos = jnp.arange(SEQUENCE_LENGTH, dtype=jnp.int32)

    def attend(index):
        begin = (index * q_block).astype(jnp.int32)
        q_rows = lax.dynamic_slice_in_dim(heads_q, begin, q_block, 0).astype(jnp.float32)
        q_gate = lax.dynamic_slice_in_dim(gate_cache, begin, q_block, 0)
        score = jnp.einsum('qgjd,kgd->gjqk', q_rows, keys_f) * HD ** (-0.5)
        score = score + q_gate.T.reshape(KVH, group, q_block, 1) - key_gate
        q_pos = begin + jnp.arange(q_block, dtype=jnp.int32)
        mask = key_pos[None, :] <= q_pos[:, None]
        score = jnp.where(mask, score, -1e+30)
        row_max = lax.optimization_barrier(jnp.max(score, axis=-1))
        weight = jnp.where(mask, jnp.exp(score - row_max[..., None]), 0.0)
        row_sum = lax.optimization_barrier(jnp.sum(weight, axis=-1))
        weight_bf = lax.optimization_barrier(weight.astype(jnp.bfloat16)).astype(jnp.float32)
        summed = jnp.einsum('gjqk,kgd->gjqd', weight_bf, values_f) / row_sum[..., None]
        out = summed.transpose(2, 0, 1, 3).reshape(q_block, QH * HD).astype(jnp.bfloat16)
        lse = (row_max + jnp.log(row_sum)).transpose(2, 0, 1).reshape(q_block, QH)
        return (out, lse)
    outs, lses = lax.map(attend, jnp.arange(n_blocks, dtype=jnp.int32))
    attn_out = outs.reshape(SEQUENCE_LENGTH, QH * HD)
    log_total = lses.reshape(SEQUENCE_LENGTH, QH)
    conv_part = CONV // N_TP
    attn_part = QH * HD // N_TP
    mixed = jnp.zeros((SEQUENCE_LENGTH, D), jnp.float32)
    for part in range(N_TP):
        term = jnp.dot(conv_out[:, part * conv_part:(part + 1) * conv_part], out_conv_w[part * conv_part:(part + 1) * conv_part], preferred_element_type=jnp.float32)
        term = term + jnp.dot(attn_out[:, part * attn_part:(part + 1) * attn_part], out_attn_w[part * attn_part:(part + 1) * attn_part], preferred_element_type=jnp.float32)
        mixed = mixed + term.astype(jnp.bfloat16).astype(jnp.float32)
    return (mixed.astype(jnp.bfloat16), log_total)
```

```python
import functools

import jax
import jax.numpy as jnp
from jax import lax
from jax.experimental import pallas as pl
from jax.experimental.pallas import tpu as pltpu
from jax.sharding import PartitionSpec as P

HD = 64
LANES = 128
MESH = pl.DeviceIdType.MESH
F32 = jnp.float32
BF16 = jnp.bfloat16


def layer_kernel(
    n_sp,
    n_tp,
    tokens_ref,
    gain_ref,
    wb_ref,
    wc_ref,
    wx_ref,
    wq_ref,
    wk_ref,
    wv_ref,
    taps_ref,
    gate_ref,
    oconv_ref,
    oattn_ref,
    mixed_ref,
    lse_ref,
    tok,
    normed,
    wconv,
    wq,
    wkv,
    kvall,
    csrc,
    halo,
    comb,
    wout,
    part,
    sib,
    fwd,
    xin,
    send_sem,
    recv_sem,
    local_sem,
):
    g = lax.axis_index("grp")
    s = lax.axis_index("sp")
    t = lax.axis_index("tp")
    up = {"sp": lax.rem(s + 1, n_sp)}
    down = {"sp": lax.rem(s + n_sp - 1, n_sp)}
    across = {"grp": 1 - g}
    depth = wb_ref.shape[0]
    rows_own = tokens_ref.shape[0]
    count = tok.shape[0]
    conv_w = (wb_ref, wc_ref, wx_ref)
    heads = wq_ref.shape[1] // HD
    channels = wb_ref.shape[1]

    def block(index, size):
        return pl.ds(pl.multiple_of(index * size, size), size)

    def shard(by):
        return block(lax.rem(s + by + n_sp, n_sp), depth)

    local = [
        pltpu.make_async_copy(oconv_ref, wout.at[pl.ds(0, channels)], local_sem.at[0]),
        pltpu.make_async_copy(
            oattn_ref, wout.at[pl.ds(channels, heads * HD)], local_sem.at[1]
        ),
    ]
    for copy in local:
        copy.start()
    wkv[shard(0), :] = jnp.concatenate([wk_ref[...], wv_ref[...]], axis=1)

    barrier = pltpu.get_barrier_semaphore()
    for by in range(1, n_sp):
        pl.semaphore_signal(
            barrier, inc=1, device_id={"sp": lax.rem(s + by, n_sp)}, device_id_type=MESH
        )
    for by in range(1, n_tp):
        pl.semaphore_signal(
            barrier, inc=1, device_id={"tp": lax.rem(t + by, n_tp)}, device_id_type=MESH
        )
    pl.semaphore_signal(barrier, inc=1, device_id=across, device_id_type=MESH)
    pl.semaphore_wait(barrier, n_sp + n_tp - 1)

    sent = []
    used = [0]

    def send(src, dst, device):
        index = used[0]
        used[0] += 1
        copy = pltpu.make_async_remote_copy(
            src_ref=src,
            dst_ref=dst,
            send_sem=send_sem.at[index],
            recv_sem=recv_sem.at[index],
            device_id=device,
            device_id_type=MESH,
        )
        copy.start()
        sent.append(copy)
        return copy

    def conv_piece(m, by):
        return wconv.at[m, g, shard(by)]

    plus_x, minus_x = [], []
    for m in range(3):
        src = conv_w[m].at[:, block(g, LANES)]
        plus_x.append(send(src, conv_piece(m, 0), up))
        minus_x.append(send(src, conv_piece(m, 0), down))
    own_kv, own_q = wkv.at[shard(0)], wq.at[shard(0)]
    plus_kv = send(own_kv, own_kv, up)
    minus_kv = send(own_kv, own_kv, down)
    plus_q = send(wq_ref, own_q, up)
    minus_q = send(wq_ref, own_q, down)
    token_copies = [
        send(tokens_ref, tok.at[block(t, rows_own)], {"tp": lax.rem(t + by, n_tp)})
        for by in range(1, n_tp)
    ]
    tok[block(t, rows_own), :] = tokens_ref[...]
    for m in range(3):
        for h in range(2):
            wconv[m, h, shard(0), :] = conv_w[m][:, h * LANES : (h + 1) * LANES]
    wq[shard(0), :] = wq_ref[...]
    padding = jnp.zeros((gate_ref.shape[0], LANES - heads), F32)
    gate_rows = jnp.concatenate([gate_ref[...], padding], axis=1).T[:heads]

    over_y, hop_x = [], []
    for m in range(3):
        plus_x[m].wait_recv()
        over_y.append(send(conv_piece(m, -1), conv_piece(m, -1), across))
        hop_x.append(send(conv_piece(m, -1), conv_piece(m, -1), up))
        minus_x[m].wait_recv()
        over_y.append(send(conv_piece(m, 1), conv_piece(m, 1), across))

    for copy in token_copies:
        copy.wait_recv()
    square = jnp.zeros((count, 1), F32)
    width = tok.shape[1]
    step = width // 4
    for c in range(4):
        cols = slice(c * step, (c + 1) * step)
        xf = tok[:, cols].astype(F32)
        square = square + jnp.sum(xf * xf, axis=-1, keepdims=True)
        normed[:, cols] = (xf * gain_ref[:, cols]).astype(BF16)
    scale_rows = lax.rsqrt(square / width + 1e-05)

    def project(weight):
        return (
            jnp.dot(normed[...], weight, preferred_element_type=F32) * scale_rows
        ).astype(BF16)

    plus_kv.wait_recv()
    minus_kv.wait_recv()
    hop_kv = send(wkv.at[shard(1)], wkv.at[shard(1)], down)
    plus_q.wait_recv()
    minus_q.wait_recv()
    hop_q = send(wq.at[shard(1)], wq.at[shard(1)], down)
    hop_x[0].wait_recv()
    over_y.append(send(conv_piece(0, -2), conv_piece(0, -2), across))
    hop_kv.wait_recv()
    own_rows = block(s, count)
    kvall[own_rows, :] = project(wkv[...])
    kv_copies = [
        send(kvall.at[own_rows], kvall.at[own_rows], {"sp": lax.rem(s + by, n_sp)})
        for by in range(1, n_sp)
    ]
    for m in range(1, 3):
        hop_x[m].wait_recv()
        over_y.append(send(conv_piece(m, -2), conv_piece(m, -2), across))

    hop_q.wait_recv()
    query = project(wq[...]) * BF16(HD**-0.5)
    for copy in kv_copies:
        copy.wait_recv()
    keys = kvall[:, :HD]
    values = kvall[:, HD:]
    total_keys = kvall.shape[0]
    q_pos = s * count + lax.broadcasted_iota(jnp.int32, (count, total_keys), 0)
    visible = lax.broadcasted_iota(jnp.int32, (count, total_keys), 1) <= q_pos
    for h in range(heads):
        score = lax.dot_general(
            query[:, h * HD : (h + 1) * HD],
            keys,
            (((1,), (1,)), ((), ())),
            preferred_element_type=F32,
        )
        score = score + gate_ref[own_rows, h : h + 1] - gate_rows[h : h + 1]
        score = jnp.where(visible, score, -1e30)
        row_max = jnp.max(score, axis=-1, keepdims=True)
        weight = jnp.exp(score - row_max)
        row_sum = jnp.sum(weight, axis=-1, keepdims=True)
        out = jnp.dot(weight.astype(BF16), values, preferred_element_type=F32)
        comb[:, channels + h * HD : channels + (h + 1) * HD] = (out / row_sum).astype(BF16)
        lse_ref[:, h : h + 1] = row_max + jnp.log(row_sum)

    for copy in over_y:
        copy.wait_recv()
    gates = []
    tail = halo.shape[0]
    for h in range(2):
        cols = slice(h * LANES, (h + 1) * LANES)
        gates.append(project(wconv[0, h]))
        gate_c = project(wconv[1, h]).astype(F32)
        csrc[:, cols] = (gate_c * project(wconv[2, h]).astype(F32)).astype(BF16)
    halo_copy = send(csrc.at[pl.ds(count - tail, tail)], halo, up)
    halo_copy.wait_recv()
    taps = taps_ref.shape[0]
    before = jnp.where(s > 0, halo[...].astype(F32), 0.0)
    source = csrc[...].astype(F32)
    filtered = jnp.zeros((count, channels), F32)
    for tap in range(taps):
        back = taps - 1 - tap
        moved = source
        if back:
            moved = jnp.concatenate([before[tail - back :], source[: count - back]], axis=0)
        filtered = filtered + taps_ref[tap : tap + 1, :] * moved
    for h in range(2):
        cols = slice(h * LANES, (h + 1) * LANES)
        comb[:, cols] = (gates[h].astype(F32) * filtered[:, cols]).astype(BF16)

    for copy in local:
        copy.wait()
    sibling = t + 1 - 2 * lax.rem(t, 2)
    far = lax.rem(t + 2, n_tp)
    far_sibling = lax.rem(sibling + 2, n_tp)
    chunks = 4
    wide = width // chunks
    near_copies, far_copies = [], []

    def relay(c):
        cols = pl.ds(c * wide, wide)
        for copy in near_copies[c]:
            copy.wait_recv()
        pair = part[far, :, cols].astype(F32) + sib[1, :, cols].astype(F32)
        fwd[:, cols] = pair.astype(BF16)
        far_copies.append(send(fwd.at[:, cols], xin.at[:, cols], {"tp": far}))

    for c in range(chunks):
        cols = pl.ds(c * wide, wide)
        term = jnp.dot(comb[...], wout[:, cols], preferred_element_type=F32).astype(BF16)
        for j in range(n_tp):
            part[j, :, cols] = term[j * rows_own : (j + 1) * rows_own]
        near_copies.append(
            [
                send(part.at[far_sibling, :, cols], sib.at[1, :, cols], {"tp": sibling}),
                send(part.at[sibling, :, cols], sib.at[0, :, cols], {"tp": sibling}),
            ]
        )
        if c:
            relay(c - 1)
    relay(chunks - 1)
    for c in range(chunks):
        cols = pl.ds(c * wide, wide)
        far_copies[c].wait_recv()
        whole = part[t, :, cols].astype(F32) + sib[0, :, cols].astype(F32)
        mixed_ref[:, cols] = (whole + xin[:, cols].astype(F32)).astype(BF16)
    for copy in sent:
        copy.wait_send()


COPIES = 64


def in_one_kernel(
    n_sp,
    n_tp,
    tokens,
    norm_gain,
    conv_b_w,
    conv_c_w,
    conv_x_w,
    query_w,
    key_w,
    value_w,
    conv_taps,
    gate_cache,
    out_conv_w,
    out_attn_w,
):
    rows, width = tokens.shape
    count = rows * n_tp
    depth, channels = conv_b_w.shape
    q_width = query_w.shape[1]
    heads = gate_cache.shape[1]
    kv_width = key_w.shape[1] + value_w.shape[1]
    total = gate_cache.shape[0]
    vmem = pl.BlockSpec(memory_space=pltpu.VMEM)
    hbm = pl.BlockSpec(memory_space=pl.ANY)
    out_rows = out_conv_w.shape[0] + out_attn_w.shape[0]
    return pl.pallas_call(
        functools.partial(layer_kernel, n_sp, n_tp),
        out_shape=(
            jax.ShapeDtypeStruct((rows, width), BF16),
            jax.ShapeDtypeStruct((count, heads), F32),
        ),
        in_specs=[vmem] * 10 + [hbm] * 2,
        out_specs=(vmem, vmem),
        scratch_shapes=[
            pltpu.VMEM((count, width), BF16),
            pltpu.VMEM((count, width), BF16),
            pltpu.VMEM((3, channels // LANES, width, LANES), BF16),
            pltpu.VMEM((width, q_width), BF16),
            pltpu.VMEM((width, kv_width), BF16),
            pltpu.VMEM((total, kv_width), BF16),
            pltpu.VMEM((count, channels), BF16),
            pltpu.VMEM((16, channels), BF16),
            pltpu.VMEM((count, channels + q_width), BF16),
            pltpu.VMEM((out_rows, width), BF16),
            pltpu.VMEM((n_tp, rows, width), BF16),
            pltpu.VMEM((2, rows, width), BF16),
            pltpu.VMEM((rows, width), BF16),
            pltpu.VMEM((rows, width), BF16),
            pltpu.SemaphoreType.DMA((COPIES,)),
            pltpu.SemaphoreType.DMA((COPIES,)),
            pltpu.SemaphoreType.DMA((2,)),
        ],
        compiler_params=pltpu.CompilerParams(
            collective_id=0, has_side_effects=True, vmem_limit_bytes=56 * 1024 * 1024
        ),
    )(
        tokens,
        norm_gain.reshape(1, width),
        conv_b_w,
        conv_c_w,
        conv_x_w,
        query_w,
        key_w,
        value_w,
        conv_taps,
        gate_cache,
        out_conv_w,
        out_attn_w,
    )


def passed_along(value, axis, by):
    count = lax.axis_size(axis)
    pairs = [(i, i + by) for i in range(count) if 0 <= i + by < count]
    return lax.ppermute(value, axis, pairs)


def on_device(
    tokens,
    norm_gain,
    conv_b_w,
    conv_c_w,
    conv_x_w,
    query_w,
    key_w,
    value_w,
    conv_taps,
    gate_cache,
    out_conv_w,
    out_attn_w,
):
    rows = lax.all_gather(tokens, "tp", axis=0, tiled=True)
    count = rows.shape[0]
    xf = rows.astype(jnp.float32)
    scale_rows = lax.rsqrt(jnp.mean(xf * xf, axis=-1, keepdims=True) + 1e-05)
    normed = (xf * norm_gain).astype(jnp.bfloat16)

    def contract_all(pieces):
        width = pieces[0].shape[0]
        return tuple(
            (jnp.dot(normed, piece, preferred_element_type=jnp.float32) for piece in pieces)
        )

    conv_sums = contract_all(
        (
            lax.all_gather(conv_b_w, "sp", axis=0, tiled=True),
            lax.all_gather(conv_c_w, "sp", axis=0, tiled=True),
            lax.all_gather(conv_x_w, "sp", axis=0, tiled=True),
        )
    )
    attn_sums = contract_all(
        (
            lax.all_gather(query_w, "sp", axis=0, tiled=True),
            lax.all_gather(key_w, "sp", axis=0, tiled=True),
            lax.all_gather(value_w, "sp", axis=0, tiled=True),
        )
    )
    sums = conv_sums + attn_sums
    gate_b, gate_c, conv_in, query, key, value = [
        (total * scale_rows).astype(jnp.bfloat16) for total in sums
    ]
    taps = conv_taps.shape[0]
    channels = conv_in.shape[1]
    conv_src = (gate_c.astype(jnp.float32) * conv_in.astype(jnp.float32)).astype(jnp.bfloat16)
    earlier = passed_along(conv_src[count - (taps - 1) :], "sp", 1)
    padded = jnp.concatenate([earlier, conv_src], axis=0)
    filtered = jnp.zeros((count, channels), jnp.float32)
    for tap in range(taps):
        filtered = filtered + conv_taps[tap][None, :] * padded[tap : tap + count].astype(
            jnp.float32
        )
    conv_out = (gate_b.astype(jnp.float32) * filtered).astype(jnp.bfloat16)
    heads_dev = gate_cache.shape[1]
    kv_dev = key.shape[1] // HD
    group = heads_dev // kv_dev
    half = count // 2
    sp_index = lax.axis_index("sp")
    own_start = sp_index * count
    scale = HD ** (-0.5)
    later_query = query[half:]
    later_start = own_start + half

    def prepare(q_rows, begin):
        heads_q = q_rows.reshape(half, kv_dev, group, HD)
        q_gate = lax.dynamic_slice_in_dim(gate_cache, begin, half, 0).T.reshape(
            kv_dev, group, half, 1
        )
        q_pos = begin + jnp.arange(half, dtype=jnp.int32)
        return (heads_q, q_gate, q_pos)

    sides = (prepare(query[:half], own_start), prepare(later_query, later_start))

    def absorb(carry, side, key_rows, value_rows, begin):
        heads_q, q_gate, q_pos = side
        run_max, run_sum, acc = carry
        width = key_rows.shape[0]
        key_heads = key_rows.reshape(width, kv_dev, HD)
        value_heads = value_rows.reshape(width, kv_dev, HD)
        score = (
            jnp.einsum("qgjd,kgd->gjqk", heads_q, key_heads, preferred_element_type=jnp.float32)
            * scale
        )
        key_gate = lax.dynamic_slice_in_dim(gate_cache, begin, width, 0).T.reshape(
            kv_dev, group, 1, width
        )
        score = score + q_gate - key_gate
        mask = (begin + jnp.arange(width, dtype=jnp.int32))[None, :] <= q_pos[:, None]
        score = jnp.where(mask, score, -1e30)
        new_max = jnp.maximum(run_max, jnp.max(score, axis=-1))
        weight = jnp.where(mask, jnp.exp(score - new_max[..., None]), 0.0)
        factor = jnp.exp(run_max - new_max)
        new_sum = run_sum * factor + jnp.sum(weight, axis=-1)
        product = jnp.einsum(
            "gjqk,kgd->gjqd",
            weight.astype(jnp.bfloat16),
            value_heads,
            preferred_element_type=jnp.float32,
        )
        return (new_max, new_sum, acc * factor[..., None] + product)

    def guarded(carry, side, key_rows, value_rows, begin):

        def visit_rows(state):
            return absorb(state, side, key_rows, value_rows, begin)

        def keep(state):
            return state

        return lax.cond(begin <= side[2][half - 1], visit_rows, keep, carry)

    def absorb_both(carry, key_rows, value_rows, begin):
        return (
            guarded(carry[0], sides[0], key_rows, value_rows, begin),
            guarded(carry[1], sides[1], key_rows, value_rows, begin),
        )

    def fresh():
        return (
            jnp.full((kv_dev, group, half), -1e30, jnp.float32),
            jnp.zeros((kv_dev, group, half), jnp.float32),
            jnp.zeros((kv_dev, group, half, HD), jnp.float32),
        )

    key_rows = lax.all_gather(key, "sp", axis=0, tiled=True)
    value_rows = lax.all_gather(value, "sp", axis=0, tiled=True)
    width = key_rows.shape[0]
    step = 512
    key_blocks = key_rows.reshape(width // step, step, key_rows.shape[1])
    value_blocks = value_rows.reshape(width // step, step, value_rows.shape[1])
    firsts = step * jnp.arange(width // step, dtype=jnp.int32)

    def visit(state, inputs):
        return (absorb_both(state, inputs[0], inputs[1], inputs[2]), None)

    result, unused = lax.scan(visit, (fresh(), fresh()), (key_blocks, value_blocks, firsts))

    def finish(state):
        run_max, run_sum, acc = state
        out = (
            (acc / run_sum[..., None])
            .transpose(2, 0, 1, 3)
            .reshape(half, heads_dev * HD)
            .astype(jnp.bfloat16)
        )
        lse = (run_max + jnp.log(run_sum)).transpose(2, 0, 1).reshape(half, heads_dev)
        return (out, lse)

    early_out, early_lse = finish(result[0])
    later_out, later_lse = finish(result[1])
    attn_out = jnp.concatenate([early_out, later_out], axis=0)
    log_total = jnp.concatenate([early_lse, later_lse], axis=0)
    term = jnp.dot(conv_out, out_conv_w, preferred_element_type=jnp.float32)
    mixed = lax.psum_scatter(
        (term + jnp.dot(attn_out, out_attn_w, preferred_element_type=jnp.float32)).astype(
            jnp.bfloat16
        ),
        "tp",
        scatter_dimension=0,
        tiled=True,
    )
    return (mixed, log_total)


def solution(mesh):
    placed = (
        P(("grp", "sp", "tp"), None),
        P(),
        P("sp", "tp"),
        P("sp", "tp"),
        P("sp", "tp"),
        P("sp", "tp"),
        P("sp", "tp"),
        P("sp", "tp"),
        P(None, "tp"),
        P("grp", "tp"),
        P("tp", None),
        P("tp", None),
    )
    sizes = dict(mesh.shape)

    def on_one(*args):
        channels, key_width = args[2].shape[1], args[6].shape[1]
        grid = (sizes["grp"], sizes["sp"], sizes["tp"])
        if grid == (2, 4, 4) and channels == 2 * LANES and key_width == HD:
            return in_one_kernel(sizes["sp"], sizes["tp"], *args)
        return on_device(*args)

    return jax.shard_map(
        on_one,
        mesh=mesh,
        in_specs=placed,
        out_specs=(P(("grp", "sp", "tp"), None), P(("grp", "sp"), "tp")),
        check_vma=False,
    )
```

```python
import functools

import jax
import jax.numpy as jnp
from jax import lax
from jax.experimental import pallas as pl
from jax.experimental.pallas import tpu as pltpu
from jax.sharding import PartitionSpec as P

HD = 64
LANES = 128
MESH = pl.DeviceIdType.MESH
F32 = jnp.float32
BF16 = jnp.bfloat16


def layer_kernel(
    n_sp,
    n_tp,
    tokens_ref,
    gain_ref,
    wb_ref,
    wc_ref,
    wx_ref,
    wq_ref,
    wk_ref,
    wv_ref,
    taps_ref,
    gate_ref,
    oconv_ref,
    oattn_ref,
    mixed_ref,
    lse_ref,
    tok,
    normed,
    packed,
    wmain,
    wkv,
    proj,
    outs,
    comb,
    lse_out,
    lse_in,
    wout,
    part,
    sib,
    fwd,
    xin,
    send_sem,
    tok_sem,
    main_sem,
    kv_sem,
    out_sem,
    sum_sem,
    local_sem,
):
    g = lax.axis_index("grp")
    s = lax.axis_index("sp")
    t = lax.axis_index("tp")
    across = {"grp": 1 - g}
    sibling = t + 1 - 2 * lax.rem(t, 2)
    far = lax.rem(t + 2, n_tp)
    far_sibling = lax.rem(sibling + 2, n_tp)
    depth = wb_ref.shape[0]
    half = depth // 2
    rows_own, width = tokens_ref.shape
    count = rows_own * n_tp
    total = count * n_sp
    ch = wb_ref.shape[1] // n_sp

    def block(index, size):
        return pl.ds(pl.multiple_of(index * size, size), size)

    local = []
    for d in range(n_sp):
        for k, ref in ((0, oconv_ref), (1, oattn_ref)):
            local.append(
                pltpu.make_async_copy(
                    ref.at[pl.ds(d * ch, ch)],
                    wout.at[pl.ds((2 * d + k) * ch, ch)],
                    local_sem.at[2 * d + k],
                )
            )
    for copy in local:
        copy.start()

    barrier = pltpu.get_barrier_semaphore()
    for by in range(1, n_sp):
        pl.semaphore_signal(
            barrier, inc=1, device_id={"sp": lax.rem(s + by, n_sp)}, device_id_type=MESH
        )
    for by in range(1, n_tp):
        pl.semaphore_signal(
            barrier, inc=1, device_id={"tp": lax.rem(t + by, n_tp)}, device_id_type=MESH
        )
    pl.semaphore_signal(barrier, inc=1, device_id=across, device_id_type=MESH)
    pl.semaphore_wait(barrier, n_sp + n_tp - 1)

    used = [0]
    sent = []

    def send(src, dst, arrival, device, when=None):
        index = used[0]
        used[0] += 1
        copy = pltpu.make_async_remote_copy(
            src_ref=src,
            dst_ref=dst,
            send_sem=send_sem.at[index],
            recv_sem=arrival,
            device_id=device,
            device_id_type=MESH,
        )
        sent.append((copy, when))
        if when is None:
            copy.start()
        else:
            pl.when(when)(copy.start)
        return copy

    def arrived(ref, arrival):
        pltpu.make_async_remote_copy(
            src_ref=ref,
            dst_ref=ref,
            send_sem=send_sem.at[0],
            recv_sem=arrival,
            device_id=across,
            device_id_type=MESH,
        ).wait_recv()

    def both(a, b):
        return b if a is None else jnp.logical_and(a, b)

    def tok_block(z, x):
        return tok.at[block(z * n_tp + x, rows_own)]

    def tok_spread(src, z, step, when):
        arrival = tok_sem.at[z * n_tp + t]
        dst = tok_block(z, t)
        if step >= 0:
            send(src, dst, arrival, {"sp": lax.rem(s + 1, n_sp)}, both(when, s < n_sp - 1))
        if step <= 0:
            send(src, dst, arrival, {"sp": lax.rem(s + n_sp - 1, n_sp)}, both(when, s > 0))
        send(src, dst, arrival, {"tp": far}, when)
        send(src, dst, arrival, {"tp": sibling}, when)

    def tok_round(h):
        for step in (1, -1):
            z = lax.rem(s - step * h + n_sp, n_sp)
            exists = (s >= h) if step > 0 else (s + h < n_sp)

            @pl.when(exists)
            def _(z=z):
                arrived(tok_block(z, t), tok_sem.at[z * n_tp + t])

            tok_spread(tok_block(z, t), z, step, exists)

    def tok_far(z):
        arrival = tok_sem.at[z * n_tp + far]
        arrived(tok_block(z, far), arrival)
        send(tok_block(z, far), tok_block(z, far), arrival, {"tp": sibling})

    def main_rows(z, g_half):
        return wmain.at[block(2 * z + g_half, half)]

    def kv_rows(z, g_half):
        return wkv.at[block(2 * z + g_half, half)]

    def weights_over(by):
        z = lax.rem(s + by, n_sp)
        arrived(main_rows(z, g), main_sem.at[z])
        send(main_rows(z, g), main_rows(z, g), main_sem.at[n_sp + z], across)
        arrived(kv_rows(z, g), kv_sem.at[z])
        send(kv_rows(z, g), kv_rows(z, g), kv_sem.at[n_sp + z], across)

    tok_spread(tokens_ref, s, 0, None)
    tok[block(s * n_tp + t, rows_own), :] = tokens_ref[...]
    for d in range(n_sp):
        cols = slice(d * ch, (d + 1) * ch)
        packed[d, :, : 2 * ch] = jnp.concatenate([wb_ref[:, cols], wc_ref[:, cols]], axis=1)
        packed[d, :, 2 * ch :] = jnp.concatenate([wx_ref[:, cols], wq_ref[:, cols]], axis=1)
    stacked = jnp.concatenate([wk_ref[...], wv_ref[...]], axis=0).astype(F32)
    wkv[block(s, depth), :] = stacked.T.astype(BF16)
    wmain[block(s, depth), :] = packed[s]

    tok_round(1)
    for by in (2, 1, 3):
        d = lax.rem(s + by, n_sp)
        send(packed.at[d, block(g, half)], main_rows(s, g), main_sem.at[s], {"sp": d})
        send(kv_rows(s, g), kv_rows(s, g), kv_sem.at[s], {"sp": d})
    tok_far(s)
    tok_round(2)
    for z_by in (1, 3):
        weights_over(z_by)
    tok_round(3)
    weights_over(2)
    for by in (1, 3, 2):
        tok_far(lax.rem(s + by, n_sp))
    for by in range(n_sp):
        z = lax.rem(s + by, n_sp)
        arrived(tok_block(z, sibling), tok_sem.at[z * n_tp + sibling])
        arrived(tok_block(z, far_sibling), tok_sem.at[z * n_tp + far_sibling])

    def normalize(i, unused):
        rows = block(i, rows_own)
        xf = tok[rows, :].astype(F32)
        square = jnp.sum(xf * xf, axis=-1, keepdims=True)
        normed[rows, :] = (xf * gain_ref[...]).astype(BF16)
        scale = lax.rsqrt(square / width + 1e-05)
        proj[rows, :] = jnp.broadcast_to(scale, (rows_own, proj.shape[1]))
        return unused

    lax.fori_loop(0, n_sp * n_tp, normalize, 0)
    scale_rows = proj[:, :1]
    gate_row = gate_ref[pl.ds(s, 1), :]
    gate_column = jnp.broadcast_to(gate_row, (LANES, total)).T[:, :1]
    taps = taps_ref.shape[0]
    taps_own = jnp.zeros((taps, ch), F32)
    for d in range(n_sp):
        taps_own = jnp.where(s == d, taps_ref[:, d * ch : (d + 1) * ch], taps_own)

    for by in range(1, n_sp):
        z = lax.rem(s + by, n_sp)
        arrived(main_rows(z, 1 - g), main_sem.at[n_sp + z])
        arrived(kv_rows(z, 1 - g), kv_sem.at[n_sp + z])

    def project(weight):
        return (
            jnp.dot(normed[...], weight, preferred_element_type=F32) * scale_rows
        ).astype(BF16)

    main = project(wmain[...])
    kv = project(wkv[...])
    gate_b = main[:, :ch].astype(F32)
    conv_src = main[:, ch : 2 * ch].astype(F32) * main[:, 2 * ch : 3 * ch].astype(F32)
    conv_src = conv_src.astype(BF16).astype(F32)
    filtered = jnp.zeros((total, ch), F32)
    for tap in range(taps):
        back = taps - 1 - tap
        moved = conv_src
        if back:
            moved = jnp.concatenate([jnp.zeros((back, ch), F32), conv_src[: total - back]], axis=0)
        filtered = filtered + taps_own[tap : tap + 1] * moved
    conv_out = (gate_b * filtered).astype(BF16)
    query = main[:, 3 * ch :] * BF16(HD**-0.5)
    keys, values = kv[:, :HD], kv[:, HD:]
    for d in reversed(range(n_sp)):
        rows = slice(d * count, (d + 1) * count)
        seen = (d + 1) * count
        score = lax.dot_general(
            query[rows],
            keys[:seen],
            (((1,), (1,)), ((), ())),
            preferred_element_type=F32,
        )
        score = score + gate_column[rows] - gate_row[:, :seen]
        q_pos = d * count + lax.broadcasted_iota(jnp.int32, (count, seen), 0)
        visible = lax.broadcasted_iota(jnp.int32, (count, seen), 1) <= q_pos
        score = jnp.where(visible, score, -1e30)
        row_max = jnp.max(score, axis=-1, keepdims=True)
        weight = jnp.exp(score - row_max)
        row_sum = jnp.sum(weight, axis=-1, keepdims=True)
        out = jnp.dot(weight.astype(BF16), values[:seen], preferred_element_type=F32)
        attn_out = (out / row_sum).astype(BF16)
        outs[d] = jnp.concatenate([conv_out[rows], attn_out], axis=1)
        logs = jnp.broadcast_to(row_max + jnp.log(row_sum), (count, LANES)).T
        lse_out[d] = logs[: lse_out.shape[1]]
        other = s != d
        send(outs.at[d], comb.at[s], out_sem.at[s], {"sp": d}, other)
        send(lse_out.at[d], lse_in.at[s], out_sem.at[n_sp + s], {"sp": d}, other)
    comb[s] = outs[s]
    lse_in[s] = lse_out[s]
    for copy in local:
        copy.wait()
    for by in range(1, n_sp):
        z = lax.rem(s + by, n_sp)
        arrived(comb.at[z], out_sem.at[z])
        arrived(lse_in.at[z], out_sem.at[n_sp + z])
    for d in range(n_sp):
        lse_ref[d : d + 1, :] = lse_in[d, :1]

    gathered = jnp.concatenate([comb[d] for d in range(n_sp)], axis=1)
    chunks = 4
    wide = width // chunks

    def relay(c):
        cols = pl.ds(c * wide, wide)
        for k in range(2):
            arrived(sib.at[k, :, cols], sum_sem.at[3 * c + k])
        pair = part[far, :, cols].astype(F32) + sib[1, :, cols].astype(F32)
        fwd[:, cols] = pair.astype(BF16)
        send(fwd.at[:, cols], xin.at[:, cols], sum_sem.at[3 * c + 2], {"tp": far})

    for c in range(chunks):
        cols = pl.ds(c * wide, wide)
        term = jnp.dot(gathered, wout[:, cols], preferred_element_type=F32).astype(BF16)
        for j in range(n_tp):
            part[j, :, cols] = term[j * rows_own : (j + 1) * rows_own]
        for k, owner in ((1, far_sibling), (0, sibling)):
            send(
                part.at[owner, :, cols],
                sib.at[k, :, cols],
                sum_sem.at[3 * c + k],
                {"tp": sibling},
            )
        if c:
            relay(c - 1)
    relay(chunks - 1)
    for c in range(chunks):
        cols = pl.ds(c * wide, wide)
        arrived(xin.at[:, cols], sum_sem.at[3 * c + 2])
        whole = part[t, :, cols].astype(F32) + sib[0, :, cols].astype(F32)
        mixed_ref[:, cols] = (whole + xin[:, cols].astype(F32)).astype(BF16)
    for copy, when in sent:
        if when is None:
            copy.wait_send()
        else:
            pl.when(when)(copy.wait_send)


COPIES = 96


def in_one_kernel(
    n_sp,
    n_tp,
    tokens,
    norm_gain,
    conv_b_w,
    conv_c_w,
    conv_x_w,
    query_w,
    key_w,
    value_w,
    conv_taps,
    gate_cache,
    out_conv_w,
    out_attn_w,
):
    rows, width = tokens.shape
    count = rows * n_tp
    depth, channels = conv_b_w.shape
    heads = gate_cache.shape[1]
    kv_width = key_w.shape[1] + value_w.shape[1]
    total = gate_cache.shape[0]
    main_width = (3 * channels + query_w.shape[1]) // n_sp
    pair_width = (channels + query_w.shape[1]) // n_sp
    vmem = pl.BlockSpec(memory_space=pltpu.VMEM)
    hbm = pl.BlockSpec(memory_space=pl.ANY)
    out_rows = out_conv_w.shape[0] + out_attn_w.shape[0]
    dma = pltpu.SemaphoreType.DMA
    mixed, log_rows = pl.pallas_call(
        functools.partial(layer_kernel, n_sp, n_tp),
        out_shape=(
            jax.ShapeDtypeStruct((rows, width), BF16),
            jax.ShapeDtypeStruct((heads, count), F32),
        ),
        in_specs=[vmem] * 10 + [hbm] * 2,
        out_specs=(vmem, vmem),
        scratch_shapes=[
            pltpu.VMEM((total, width), BF16),
            pltpu.VMEM((total, width), BF16),
            pltpu.VMEM((n_sp, depth, main_width), BF16),
            pltpu.VMEM((width, main_width), BF16),
            pltpu.VMEM((width, kv_width), BF16),
            pltpu.VMEM((total, LANES), F32),
            pltpu.VMEM((n_sp, count, pair_width), BF16),
            pltpu.VMEM((n_sp, count, pair_width), BF16),
            pltpu.VMEM((n_sp, 8, count), F32),
            pltpu.VMEM((n_sp, 8, count), F32),
            pltpu.VMEM((out_rows, width), BF16),
            pltpu.VMEM((n_tp, rows, width), BF16),
            pltpu.VMEM((2, rows, width), BF16),
            pltpu.VMEM((rows, width), BF16),
            pltpu.VMEM((rows, width), BF16),
            dma((COPIES,)),
            dma((n_sp * n_tp,)),
            dma((2 * n_sp,)),
            dma((2 * n_sp,)),
            dma((2 * n_sp,)),
            dma((12,)),
            dma((2 * n_sp,)),
        ],
        compiler_params=pltpu.CompilerParams(
            collective_id=0, has_side_effects=True, vmem_limit_bytes=60 * 1024 * 1024
        ),
    )(
        tokens,
        norm_gain.reshape(1, width),
        conv_b_w,
        conv_c_w,
        conv_x_w,
        query_w,
        key_w.T,
        value_w.T,
        conv_taps,
        gate_cache.T,
        out_conv_w,
        out_attn_w,
    )
    return mixed, log_rows.T


def passed_along(value, axis, by):
    count = lax.axis_size(axis)
    pairs = [(i, i + by) for i in range(count) if 0 <= i + by < count]
    return lax.ppermute(value, axis, pairs)


def on_device(
    tokens,
    norm_gain,
    conv_b_w,
    conv_c_w,
    conv_x_w,
    query_w,
    key_w,
    value_w,
    conv_taps,
    gate_cache,
    out_conv_w,
    out_attn_w,
):
    rows = lax.all_gather(tokens, "tp", axis=0, tiled=True)
    count = rows.shape[0]
    xf = rows.astype(jnp.float32)
    scale_rows = lax.rsqrt(jnp.mean(xf * xf, axis=-1, keepdims=True) + 1e-05)
    normed = (xf * norm_gain).astype(jnp.bfloat16)

    def contract_all(pieces):
        width = pieces[0].shape[0]
        return tuple(
            (jnp.dot(normed, piece, preferred_element_type=jnp.float32) for piece in pieces)
        )

    conv_sums = contract_all(
        (
            lax.all_gather(conv_b_w, "sp", axis=0, tiled=True),
            lax.all_gather(conv_c_w, "sp", axis=0, tiled=True),
            lax.all_gather(conv_x_w, "sp", axis=0, tiled=True),
        )
    )
    attn_sums = contract_all(
        (
            lax.all_gather(query_w, "sp", axis=0, tiled=True),
            lax.all_gather(key_w, "sp", axis=0, tiled=True),
            lax.all_gather(value_w, "sp", axis=0, tiled=True),
        )
    )
    sums = conv_sums + attn_sums
    gate_b, gate_c, conv_in, query, key, value = [
        (total * scale_rows).astype(jnp.bfloat16) for total in sums
    ]
    taps = conv_taps.shape[0]
    channels = conv_in.shape[1]
    conv_src = (gate_c.astype(jnp.float32) * conv_in.astype(jnp.float32)).astype(jnp.bfloat16)
    earlier = passed_along(conv_src[count - (taps - 1) :], "sp", 1)
    padded = jnp.concatenate([earlier, conv_src], axis=0)
    filtered = jnp.zeros((count, channels), jnp.float32)
    for tap in range(taps):
        filtered = filtered + conv_taps[tap][None, :] * padded[tap : tap + count].astype(
            jnp.float32
        )
    conv_out = (gate_b.astype(jnp.float32) * filtered).astype(jnp.bfloat16)
    heads_dev = gate_cache.shape[1]
    kv_dev = key.shape[1] // HD
    group = heads_dev // kv_dev
    half = count // 2
    sp_index = lax.axis_index("sp")
    own_start = sp_index * count
    scale = HD ** (-0.5)
    later_query = query[half:]
    later_start = own_start + half

    def prepare(q_rows, begin):
        heads_q = q_rows.reshape(half, kv_dev, group, HD)
        q_gate = lax.dynamic_slice_in_dim(gate_cache, begin, half, 0).T.reshape(
            kv_dev, group, half, 1
        )
        q_pos = begin + jnp.arange(half, dtype=jnp.int32)
        return (heads_q, q_gate, q_pos)

    sides = (prepare(query[:half], own_start), prepare(later_query, later_start))

    def absorb(carry, side, key_rows, value_rows, begin):
        heads_q, q_gate, q_pos = side
        run_max, run_sum, acc = carry
        width = key_rows.shape[0]
        key_heads = key_rows.reshape(width, kv_dev, HD)
        value_heads = value_rows.reshape(width, kv_dev, HD)
        score = (
            jnp.einsum("qgjd,kgd->gjqk", heads_q, key_heads, preferred_element_type=jnp.float32)
            * scale
        )
        key_gate = lax.dynamic_slice_in_dim(gate_cache, begin, width, 0).T.reshape(
            kv_dev, group, 1, width
        )
        score = score + q_gate - key_gate
        mask = (begin + jnp.arange(width, dtype=jnp.int32))[None, :] <= q_pos[:, None]
        score = jnp.where(mask, score, -1e30)
        new_max = jnp.maximum(run_max, jnp.max(score, axis=-1))
        weight = jnp.where(mask, jnp.exp(score - new_max[..., None]), 0.0)
        factor = jnp.exp(run_max - new_max)
        new_sum = run_sum * factor + jnp.sum(weight, axis=-1)
        product = jnp.einsum(
            "gjqk,kgd->gjqd",
            weight.astype(jnp.bfloat16),
            value_heads,
            preferred_element_type=jnp.float32,
        )
        return (new_max, new_sum, acc * factor[..., None] + product)

    def guarded(carry, side, key_rows, value_rows, begin):

        def visit_rows(state):
            return absorb(state, side, key_rows, value_rows, begin)

        def keep(state):
            return state

        return lax.cond(begin <= side[2][half - 1], visit_rows, keep, carry)

    def absorb_both(carry, key_rows, value_rows, begin):
        return (
            guarded(carry[0], sides[0], key_rows, value_rows, begin),
            guarded(carry[1], sides[1], key_rows, value_rows, begin),
        )

    def fresh():
        return (
            jnp.full((kv_dev, group, half), -1e30, jnp.float32),
            jnp.zeros((kv_dev, group, half), jnp.float32),
            jnp.zeros((kv_dev, group, half, HD), jnp.float32),
        )

    key_rows = lax.all_gather(key, "sp", axis=0, tiled=True)
    value_rows = lax.all_gather(value, "sp", axis=0, tiled=True)
    width = key_rows.shape[0]
    step = 512
    key_blocks = key_rows.reshape(width // step, step, key_rows.shape[1])
    value_blocks = value_rows.reshape(width // step, step, value_rows.shape[1])
    firsts = step * jnp.arange(width // step, dtype=jnp.int32)

    def visit(state, inputs):
        return (absorb_both(state, inputs[0], inputs[1], inputs[2]), None)

    result, unused = lax.scan(visit, (fresh(), fresh()), (key_blocks, value_blocks, firsts))

    def finish(state):
        run_max, run_sum, acc = state
        out = (
            (acc / run_sum[..., None])
            .transpose(2, 0, 1, 3)
            .reshape(half, heads_dev * HD)
            .astype(jnp.bfloat16)
        )
        lse = (run_max + jnp.log(run_sum)).transpose(2, 0, 1).reshape(half, heads_dev)
        return (out, lse)

    early_out, early_lse = finish(result[0])
    later_out, later_lse = finish(result[1])
    attn_out = jnp.concatenate([early_out, later_out], axis=0)
    log_total = jnp.concatenate([early_lse, later_lse], axis=0)
    term = jnp.dot(conv_out, out_conv_w, preferred_element_type=jnp.float32)
    mixed = lax.psum_scatter(
        (term + jnp.dot(attn_out, out_attn_w, preferred_element_type=jnp.float32)).astype(
            jnp.bfloat16
        ),
        "tp",
        scatter_dimension=0,
        tiled=True,
    )
    return (mixed, log_total)


def solution(mesh):
    placed = (
        P(("grp", "sp", "tp"), None),
        P(),
        P("sp", "tp"),
        P("sp", "tp"),
        P("sp", "tp"),
        P("sp", "tp"),
        P("sp", "tp"),
        P("sp", "tp"),
        P(None, "tp"),
        P("grp", "tp"),
        P("tp", None),
        P("tp", None),
    )
    sizes = dict(mesh.shape)

    def on_one(*args):
        channels, key_width = args[2].shape[1], args[6].shape[1]
        grid = (sizes["grp"], sizes["sp"], sizes["tp"])
        fits = channels == sizes["sp"] * HD and key_width == HD
        if grid == (2, 4, 4) and fits and args[9].shape[1] == sizes["sp"]:
            return in_one_kernel(sizes["sp"], sizes["tp"], *args)
        return on_device(*args)

    return jax.shard_map(
        on_one,
        mesh=mesh,
        in_specs=placed,
        out_specs=(P(("grp", "sp", "tp"), None), P(("grp", "sp"), "tp")),
        check_vma=False,
    )
```

```python
import functools

import jax
import jax.numpy as jnp
from jax import lax
from jax.experimental import pallas as pl
from jax.experimental.pallas import tpu as pltpu
from jax.sharding import PartitionSpec as P

HD = 64
LANES = 128
MESH = pl.DeviceIdType.MESH
F32 = jnp.float32
BF16 = jnp.bfloat16


def layer_kernel(
    n_sp,
    n_tp,
    tokens_ref,
    gain_ref,
    wb_hbm,
    wc_hbm,
    wx_hbm,
    wq_hbm,
    wk_hbm,
    wv_hbm,
    taps_ref,
    gate_ref,
    oconv_ref,
    oattn_ref,
    mixed_ref,
    lse_ref,
    tok,
    normed,
    packed,
    wmain,
    wkv,
    proj,
    outs,
    comb,
    lse_out,
    lse_in,
    wout,
    part,
    sib,
    fwd,
    xin,
    wb_ref,
    wc_ref,
    wx_ref,
    wq_ref,
    wk_ref,
    wv_ref,
    send_sem,
    tok_sem,
    main_sem,
    kv_sem,
    out_sem,
    sum_sem,
    local_sem,
):
    g = lax.axis_index("grp")
    s = lax.axis_index("sp")
    t = lax.axis_index("tp")
    across = {"grp": 1 - g}
    sibling = t + 1 - 2 * lax.rem(t, 2)
    far = lax.rem(t + 2, n_tp)
    far_sibling = lax.rem(sibling + 2, n_tp)
    depth = wb_hbm.shape[0]
    half = depth // 2
    rows_own, width = tokens_ref.shape
    count = rows_own * n_tp
    total = count * n_sp
    sub = rows_own // 2
    ch = wb_hbm.shape[1] // n_sp

    def block(index, size):
        return pl.ds(pl.multiple_of(index * size, size), size)

    local = []
    for d in range(n_sp):
        for k, ref in ((0, oconv_ref), (1, oattn_ref)):
            local.append(
                pltpu.make_async_copy(
                    ref.at[pl.ds(d * ch, ch)],
                    wout.at[pl.ds((2 * d + k) * ch, ch)],
                    local_sem.at[2 * d + k],
                )
            )
    weights_in = [
        pltpu.make_async_copy(src, dst, local_sem.at[2 * n_sp + k])
        for k, (src, dst) in enumerate(
            (
                (wb_hbm, wb_ref),
                (wc_hbm, wc_ref),
                (wx_hbm, wx_ref),
                (wq_hbm, wq_ref),
                (wk_hbm, wk_ref),
                (wv_hbm, wv_ref),
            )
        )
    ]
    for copy in weights_in + local:
        copy.start()

    barrier = pltpu.get_barrier_semaphore()
    for by in range(1, n_sp):
        pl.semaphore_signal(
            barrier, inc=1, device_id={"sp": lax.rem(s + by, n_sp)}, device_id_type=MESH
        )
    for by in range(1, n_tp):
        pl.semaphore_signal(
            barrier, inc=1, device_id={"tp": lax.rem(t + by, n_tp)}, device_id_type=MESH
        )
    pl.semaphore_signal(barrier, inc=1, device_id=across, device_id_type=MESH)
    pl.semaphore_wait(barrier, n_sp + n_tp - 1)

    used = [0]
    sent = []

    def send(src, dst, arrival, device, when=None):
        index = used[0]
        used[0] += 1
        copy = pltpu.make_async_remote_copy(
            src_ref=src,
            dst_ref=dst,
            send_sem=send_sem.at[index],
            recv_sem=arrival,
            device_id=device,
            device_id_type=MESH,
        )
        sent.append((copy, when))
        if when is None:
            copy.start()
        else:
            pl.when(when)(copy.start)
        return copy

    def arrived(ref, arrival):
        pltpu.make_async_remote_copy(
            src_ref=ref,
            dst_ref=ref,
            send_sem=send_sem.at[0],
            recv_sem=arrival,
            device_id=across,
            device_id_type=MESH,
        ).wait_recv()

    def both(a, b):
        return b if a is None else jnp.logical_and(a, b)

    def tok_block(z, x):
        return tok.at[block(z * n_tp + x, rows_own)]

    def tok_spread(src, z, step, when):
        arrival = tok_sem.at[z * n_tp + t]
        dst = tok_block(z, t)
        if step >= 0:
            send(src, dst, arrival, {"sp": lax.rem(s + 1, n_sp)}, both(when, s < n_sp - 1))
        if step <= 0:
            send(src, dst, arrival, {"sp": lax.rem(s + n_sp - 1, n_sp)}, both(when, s > 0))
        send(src, dst, arrival, {"tp": far}, when)
        send(src, dst, arrival, {"tp": sibling}, when)

    def tok_round(h):
        for step in (1, -1):
            z = lax.rem(s - step * h + n_sp, n_sp)
            exists = (s >= h) if step > 0 else (s + h < n_sp)

            @pl.when(exists)
            def _(z=z):
                arrived(tok_block(z, t), tok_sem.at[z * n_tp + t])

            tok_spread(tok_block(z, t), z, step, exists)

    def tok_far(z):
        arrival = tok_sem.at[z * n_tp + far]
        arrived(tok_block(z, far), arrival)
        send(tok_block(z, far), tok_block(z, far), arrival, {"tp": sibling})

    def main_rows(z, g_half):
        return wmain.at[block(2 * z + g_half, half)]

    def kv_rows(z, g_half):
        return wkv.at[block(2 * z + g_half, half)]

    def weights_out(h):
        for step in (1, -1):
            exists = (s + h < n_sp) if step > 0 else (s >= h)
            d = lax.rem(s + step * h + n_sp, n_sp)
            to = {"sp": d}
            send(kv_rows(s, g), kv_rows(s, g), kv_sem.at[s], to, exists)
            send(packed.at[d, block(g, half)], main_rows(s, g), main_sem.at[s], to, exists)

    def weights_over(h):
        for step in (1, -1):
            exists = (s >= h) if step > 0 else (s + h < n_sp)
            z = lax.rem(s - step * h + n_sp, n_sp)
            for rows, sems in ((kv_rows, kv_sem), (main_rows, main_sem)):

                @pl.when(exists)
                def _(rows=rows, sems=sems, z=z):
                    arrived(rows(z, g), sems.at[z])

                send(rows(z, g), rows(z, g), sems.at[n_sp + z], across, exists)

    tok_spread(tokens_ref, s, 0, None)
    tok[block(s * n_tp + t, rows_own), :] = tokens_ref[...]
    for copy in weights_in:
        copy.wait()
    for d in range(n_sp):
        cols = slice(d * ch, (d + 1) * ch)
        packed[d, :, : 2 * ch] = jnp.concatenate([wb_ref[:, cols], wc_ref[:, cols]], axis=1)
        packed[d, :, 2 * ch :] = jnp.concatenate([wx_ref[:, cols], wq_ref[:, cols]], axis=1)
    stacked = jnp.concatenate([wk_ref[...], wv_ref[...]], axis=0).astype(F32)
    wkv[block(s, depth), :] = stacked.T.astype(BF16)
    wmain[block(s, depth), :] = packed[s]

    for h in range(1, n_sp):
        weights_out(h)
    tok_round(1)
    tok_far(s)
    for h in range(1, n_sp):
        weights_over(h)
        if h + 1 < n_sp:
            tok_round(h + 1)
    for by in (1, 3, 2):
        tok_far(lax.rem(s + by, n_sp))
    for by in range(n_sp):
        z = lax.rem(s + by, n_sp)
        arrived(tok_block(z, sibling), tok_sem.at[z * n_tp + sibling])
        arrived(tok_block(z, far_sibling), tok_sem.at[z * n_tp + far_sibling])

    def normalize(i, unused):
        rows = block(i, rows_own)
        xf = tok[rows, :].astype(F32)
        square = jnp.sum(xf * xf, axis=-1, keepdims=True)
        normed[rows, :] = (xf * gain_ref[...]).astype(BF16)
        scale = lax.rsqrt(square / width + 1e-05)
        proj[rows, :] = jnp.broadcast_to(scale, (rows_own, proj.shape[1]))
        return unused

    lax.fori_loop(0, n_sp * n_tp, normalize, 0)
    scale_rows = proj[:, :1]
    gate_row = gate_ref[pl.ds(s, 1), :]
    gate_column = jnp.broadcast_to(gate_row, (LANES, total)).T[:, :1]
    taps = taps_ref.shape[0]
    taps_own = jnp.zeros((taps, ch), F32)
    for d in range(n_sp):
        taps_own = jnp.where(s == d, taps_ref[:, d * ch : (d + 1) * ch], taps_own)

    for by in range(1, n_sp):
        z = lax.rem(s + by, n_sp)
        arrived(main_rows(z, 1 - g), main_sem.at[n_sp + z])
        arrived(kv_rows(z, 1 - g), kv_sem.at[n_sp + z])

    def project(weight):
        return (
            jnp.dot(normed[...], weight, preferred_element_type=F32) * scale_rows
        ).astype(BF16)

    main = project(wmain[...])
    kv = project(wkv[...])
    gate_b = main[:, :ch].astype(F32)
    conv_src = main[:, ch : 2 * ch].astype(F32) * main[:, 2 * ch : 3 * ch].astype(F32)
    conv_src = conv_src.astype(BF16).astype(F32)
    filtered = jnp.zeros((total, ch), F32)
    for tap in range(taps):
        back = taps - 1 - tap
        moved = conv_src
        if back:
            moved = jnp.concatenate([jnp.zeros((back, ch), F32), conv_src[: total - back]], axis=0)
        filtered = filtered + taps_own[tap : tap + 1] * moved
    conv_out = (gate_b * filtered).astype(BF16)
    query = main[:, 3 * ch :] * BF16(HD**-0.5)
    keys, values = kv[:, :HD], kv[:, HD:]
    for d in reversed(range(n_sp)):
        rows = slice(d * count, (d + 1) * count)
        seen = (d + 1) * count
        score = lax.dot_general(
            query[rows],
            keys[:seen],
            (((1,), (1,)), ((), ())),
            preferred_element_type=F32,
        )
        score = score + gate_column[rows] - gate_row[:, :seen]
        q_pos = d * count + lax.broadcasted_iota(jnp.int32, (count, seen), 0)
        visible = lax.broadcasted_iota(jnp.int32, (count, seen), 1) <= q_pos
        score = jnp.where(visible, score, -1e30)
        row_max = jnp.max(score, axis=-1, keepdims=True)
        weight = jnp.exp(score - row_max)
        row_sum = jnp.sum(weight, axis=-1, keepdims=True)
        out = jnp.dot(weight.astype(BF16), values[:seen], preferred_element_type=F32)
        attn_out = (out / row_sum).astype(BF16)
        both_out = jnp.concatenate([conv_out[rows], attn_out], axis=1)
        for r in range(2):
            for k in range(n_tp):
                start = k * rows_own + r * sub
                outs[r, d, k * sub : (k + 1) * sub] = both_out[start : start + sub]
        logs = jnp.broadcast_to(row_max + jnp.log(row_sum), (count, LANES)).T
        lse_out[d] = logs[: lse_out.shape[1]]
        other = s != d
        send(outs.at[0, d], comb.at[0, s], out_sem.at[s], {"sp": d}, other)
    for d in range(n_sp):
        other = s != d
        send(outs.at[1, d], comb.at[1, s], out_sem.at[n_sp + s], {"sp": d}, other)
        send(lse_out.at[d], lse_in.at[s], out_sem.at[2 * n_sp + s], {"sp": d}, other)
    for r in range(2):
        comb[r, s] = outs[r, s]
    lse_in[s] = lse_out[s]
    for copy in local:
        copy.wait()

    chunks = 2
    wide = width // chunks

    def relay(r, c):
        cols = pl.ds(c * wide, wide)
        base = 3 * (chunks * r + c)
        for k in range(2):
            arrived(sib.at[r, k, :, cols], sum_sem.at[base + k])
        pair = part[r, far, :, cols].astype(F32) + sib[r, 1, :, cols].astype(F32)
        fwd[r, :, cols] = pair.astype(BF16)
        send(fwd.at[r, :, cols], xin.at[r, :, cols], sum_sem.at[base + 2], {"tp": far})

    last = None
    for r in range(2):
        for by in range(1, n_sp):
            z = lax.rem(s + by, n_sp)
            arrived(comb.at[r, z], out_sem.at[r * n_sp + z])
        gathered = jnp.concatenate([comb[r, d] for d in range(n_sp)], axis=1)
        for c in range(chunks):
            cols = pl.ds(c * wide, wide)
            term = jnp.dot(gathered, wout[:, cols], preferred_element_type=F32).astype(BF16)
            for k in range(n_tp):
                part[r, k, :, cols] = term[k * sub : (k + 1) * sub]
            for k, owner in ((1, far_sibling), (0, sibling)):
                send(
                    part.at[r, owner, :, cols],
                    sib.at[r, k, :, cols],
                    sum_sem.at[3 * (chunks * r + c) + k],
                    {"tp": sibling},
                )
            if last is not None:
                relay(*last)
            last = (r, c)
    relay(*last)
    for by in range(1, n_sp):
        z = lax.rem(s + by, n_sp)
        arrived(lse_in.at[z], out_sem.at[2 * n_sp + z])
    for d in range(n_sp):
        lse_ref[d : d + 1, :] = lse_in[d, :1]
    for r in range(2):
        for c in range(chunks):
            cols = pl.ds(c * wide, wide)
            arrived(xin.at[r, :, cols], sum_sem.at[3 * (chunks * r + c) + 2])
            whole = part[r, t, :, cols].astype(F32) + sib[r, 0, :, cols].astype(F32)
            whole = whole + xin[r, :, cols].astype(F32)
            mixed_ref[r * sub : (r + 1) * sub, cols] = whole.astype(BF16)
    for copy, when in sent:
        if when is None:
            copy.wait_send()
        else:
            pl.when(when)(copy.wait_send)


COPIES = 128


def in_one_kernel(
    n_sp,
    n_tp,
    tokens,
    norm_gain,
    conv_b_w,
    conv_c_w,
    conv_x_w,
    query_w,
    key_w,
    value_w,
    conv_taps,
    gate_cache,
    out_conv_w,
    out_attn_w,
):
    rows, width = tokens.shape
    count = rows * n_tp
    depth, channels = conv_b_w.shape
    heads = gate_cache.shape[1]
    kv_width = key_w.shape[1] + value_w.shape[1]
    total = gate_cache.shape[0]
    main_width = (3 * channels + query_w.shape[1]) // n_sp
    pair_width = (channels + query_w.shape[1]) // n_sp
    vmem = pl.BlockSpec(memory_space=pltpu.VMEM)
    hbm = pl.BlockSpec(memory_space=pl.ANY)
    out_rows = out_conv_w.shape[0] + out_attn_w.shape[0]
    dma = pltpu.SemaphoreType.DMA
    mixed, log_rows = pl.pallas_call(
        functools.partial(layer_kernel, n_sp, n_tp),
        out_shape=(
            jax.ShapeDtypeStruct((rows, width), BF16),
            jax.ShapeDtypeStruct((heads, count), F32),
        ),
        in_specs=[vmem] * 2 + [hbm] * 6 + [vmem] * 2 + [hbm] * 2,
        out_specs=(vmem, vmem),
        scratch_shapes=[
            pltpu.VMEM((total, width), BF16),
            pltpu.VMEM((total, width), BF16),
            pltpu.VMEM((n_sp, depth, main_width), BF16),
            pltpu.VMEM((width, main_width), BF16),
            pltpu.VMEM((width, kv_width), BF16),
            pltpu.VMEM((total, LANES), F32),
            pltpu.VMEM((2, n_sp, count // 2, pair_width), BF16),
            pltpu.VMEM((2, n_sp, count // 2, pair_width), BF16),
            pltpu.VMEM((n_sp, 8, count), F32),
            pltpu.VMEM((n_sp, 8, count), F32),
            pltpu.VMEM((out_rows, width), BF16),
            pltpu.VMEM((2, n_tp, rows // 2, width), BF16),
            pltpu.VMEM((2, 2, rows // 2, width), BF16),
            pltpu.VMEM((2, rows // 2, width), BF16),
            pltpu.VMEM((2, rows // 2, width), BF16),
            pltpu.VMEM(conv_b_w.shape, BF16),
            pltpu.VMEM(conv_c_w.shape, BF16),
            pltpu.VMEM(conv_x_w.shape, BF16),
            pltpu.VMEM(query_w.shape, BF16),
            pltpu.VMEM(key_w.shape[::-1], BF16),
            pltpu.VMEM(value_w.shape[::-1], BF16),
            dma((COPIES,)),
            dma((n_sp * n_tp,)),
            dma((2 * n_sp,)),
            dma((2 * n_sp,)),
            dma((3 * n_sp,)),
            dma((12,)),
            dma((2 * n_sp + 6,)),
        ],
        compiler_params=pltpu.CompilerParams(
            collective_id=0, has_side_effects=True, vmem_limit_bytes=60 * 1024 * 1024
        ),
    )(
        tokens,
        norm_gain.reshape(1, width),
        conv_b_w,
        conv_c_w,
        conv_x_w,
        query_w,
        key_w.T,
        value_w.T,
        conv_taps,
        gate_cache.T,
        out_conv_w,
        out_attn_w,
    )
    return mixed, log_rows.T


def passed_along(value, axis, by):
    count = lax.axis_size(axis)
    pairs = [(i, i + by) for i in range(count) if 0 <= i + by < count]
    return lax.ppermute(value, axis, pairs)


def on_device(
    tokens,
    norm_gain,
    conv_b_w,
    conv_c_w,
    conv_x_w,
    query_w,
    key_w,
    value_w,
    conv_taps,
    gate_cache,
    out_conv_w,
    out_attn_w,
):
    rows = lax.all_gather(tokens, "tp", axis=0, tiled=True)
    count = rows.shape[0]
    xf = rows.astype(jnp.float32)
    scale_rows = lax.rsqrt(jnp.mean(xf * xf, axis=-1, keepdims=True) + 1e-05)
    normed = (xf * norm_gain).astype(jnp.bfloat16)

    def contract_all(pieces):
        width = pieces[0].shape[0]
        return tuple(
            (jnp.dot(normed, piece, preferred_element_type=jnp.float32) for piece in pieces)
        )

    conv_sums = contract_all(
        (
            lax.all_gather(conv_b_w, "sp", axis=0, tiled=True),
            lax.all_gather(conv_c_w, "sp", axis=0, tiled=True),
            lax.all_gather(conv_x_w, "sp", axis=0, tiled=True),
        )
    )
    attn_sums = contract_all(
        (
            lax.all_gather(query_w, "sp", axis=0, tiled=True),
            lax.all_gather(key_w, "sp", axis=0, tiled=True),
            lax.all_gather(value_w, "sp", axis=0, tiled=True),
        )
    )
    sums = conv_sums + attn_sums
    gate_b, gate_c, conv_in, query, key, value = [
        (total * scale_rows).astype(jnp.bfloat16) for total in sums
    ]
    taps = conv_taps.shape[0]
    channels = conv_in.shape[1]
    conv_src = (gate_c.astype(jnp.float32) * conv_in.astype(jnp.float32)).astype(jnp.bfloat16)
    earlier = passed_along(conv_src[count - (taps - 1) :], "sp", 1)
    padded = jnp.concatenate([earlier, conv_src], axis=0)
    filtered = jnp.zeros((count, channels), jnp.float32)
    for tap in range(taps):
        filtered = filtered + conv_taps[tap][None, :] * padded[tap : tap + count].astype(
            jnp.float32
        )
    conv_out = (gate_b.astype(jnp.float32) * filtered).astype(jnp.bfloat16)
    heads_dev = gate_cache.shape[1]
    kv_dev = key.shape[1] // HD
    group = heads_dev // kv_dev
    half = count // 2
    sp_index = lax.axis_index("sp")
    own_start = sp_index * count
    scale = HD ** (-0.5)
    later_query = query[half:]
    later_start = own_start + half

    def prepare(q_rows, begin):
        heads_q = q_rows.reshape(half, kv_dev, group, HD)
        q_gate = lax.dynamic_slice_in_dim(gate_cache, begin, half, 0).T.reshape(
            kv_dev, group, half, 1
        )
        q_pos = begin + jnp.arange(half, dtype=jnp.int32)
        return (heads_q, q_gate, q_pos)

    sides = (prepare(query[:half], own_start), prepare(later_query, later_start))

    def absorb(carry, side, key_rows, value_rows, begin):
        heads_q, q_gate, q_pos = side
        run_max, run_sum, acc = carry
        width = key_rows.shape[0]
        key_heads = key_rows.reshape(width, kv_dev, HD)
        value_heads = value_rows.reshape(width, kv_dev, HD)
        score = (
            jnp.einsum("qgjd,kgd->gjqk", heads_q, key_heads, preferred_element_type=jnp.float32)
            * scale
        )
        key_gate = lax.dynamic_slice_in_dim(gate_cache, begin, width, 0).T.reshape(
            kv_dev, group, 1, width
        )
        score = score + q_gate - key_gate
        mask = (begin + jnp.arange(width, dtype=jnp.int32))[None, :] <= q_pos[:, None]
        score = jnp.where(mask, score, -1e30)
        new_max = jnp.maximum(run_max, jnp.max(score, axis=-1))
        weight = jnp.where(mask, jnp.exp(score - new_max[..., None]), 0.0)
        factor = jnp.exp(run_max - new_max)
        new_sum = run_sum * factor + jnp.sum(weight, axis=-1)
        product = jnp.einsum(
            "gjqk,kgd->gjqd",
            weight.astype(jnp.bfloat16),
            value_heads,
            preferred_element_type=jnp.float32,
        )
        return (new_max, new_sum, acc * factor[..., None] + product)

    def guarded(carry, side, key_rows, value_rows, begin):

        def visit_rows(state):
            return absorb(state, side, key_rows, value_rows, begin)

        def keep(state):
            return state

        return lax.cond(begin <= side[2][half - 1], visit_rows, keep, carry)

    def absorb_both(carry, key_rows, value_rows, begin):
        return (
            guarded(carry[0], sides[0], key_rows, value_rows, begin),
            guarded(carry[1], sides[1], key_rows, value_rows, begin),
        )

    def fresh():
        return (
            jnp.full((kv_dev, group, half), -1e30, jnp.float32),
            jnp.zeros((kv_dev, group, half), jnp.float32),
            jnp.zeros((kv_dev, group, half, HD), jnp.float32),
        )

    key_rows = lax.all_gather(key, "sp", axis=0, tiled=True)
    value_rows = lax.all_gather(value, "sp", axis=0, tiled=True)
    width = key_rows.shape[0]
    step = 512
    key_blocks = key_rows.reshape(width // step, step, key_rows.shape[1])
    value_blocks = value_rows.reshape(width // step, step, value_rows.shape[1])
    firsts = step * jnp.arange(width // step, dtype=jnp.int32)

    def visit(state, inputs):
        return (absorb_both(state, inputs[0], inputs[1], inputs[2]), None)

    result, unused = lax.scan(visit, (fresh(), fresh()), (key_blocks, value_blocks, firsts))

    def finish(state):
        run_max, run_sum, acc = state
        out = (
            (acc / run_sum[..., None])
            .transpose(2, 0, 1, 3)
            .reshape(half, heads_dev * HD)
            .astype(jnp.bfloat16)
        )
        lse = (run_max + jnp.log(run_sum)).transpose(2, 0, 1).reshape(half, heads_dev)
        return (out, lse)

    early_out, early_lse = finish(result[0])
    later_out, later_lse = finish(result[1])
    attn_out = jnp.concatenate([early_out, later_out], axis=0)
    log_total = jnp.concatenate([early_lse, later_lse], axis=0)
    term = jnp.dot(conv_out, out_conv_w, preferred_element_type=jnp.float32)
    mixed = lax.psum_scatter(
        (term + jnp.dot(attn_out, out_attn_w, preferred_element_type=jnp.float32)).astype(
            jnp.bfloat16
        ),
        "tp",
        scatter_dimension=0,
        tiled=True,
    )
    return (mixed, log_total)


def solution(mesh):
    placed = (
        P(("grp", "sp", "tp"), None),
        P(),
        P("sp", "tp"),
        P("sp", "tp"),
        P("sp", "tp"),
        P("sp", "tp"),
        P("sp", "tp"),
        P("sp", "tp"),
        P(None, "tp"),
        P("grp", "tp"),
        P("tp", None),
        P("tp", None),
    )
    sizes = dict(mesh.shape)

    def on_one(*args):
        channels, key_width = args[2].shape[1], args[6].shape[1]
        grid = (sizes["grp"], sizes["sp"], sizes["tp"])
        fits = channels == sizes["sp"] * HD and key_width == HD
        if grid == (2, 4, 4) and fits and args[9].shape[1] == sizes["sp"]:
            return in_one_kernel(sizes["sp"], sizes["tp"], *args)
        return on_device(*args)

    return jax.shard_map(
        on_one,
        mesh=mesh,
        in_specs=placed,
        out_specs=(P(("grp", "sp", "tp"), None), P(("grp", "sp"), "tp")),
        check_vma=False,
    )
```

```python
import functools

import jax
import jax.numpy as jnp
from jax import lax
from jax.experimental import pallas as pl
from jax.experimental.pallas import tpu as pltpu
from jax.sharding import PartitionSpec as P

HD = 64
LANES = 128
MESH = pl.DeviceIdType.MESH
F32 = jnp.float32
BF16 = jnp.bfloat16


def layer_kernel(
    n_sp,
    n_tp,
    tokens_ref,
    gain_ref,
    wb_hbm,
    wc_hbm,
    wx_hbm,
    wq_hbm,
    wk_hbm,
    wv_hbm,
    taps_ref,
    gate_ref,
    oconv_ref,
    oattn_ref,
    mixed_ref,
    lse_ref,
    tok,
    normed,
    packed,
    wmain,
    wkv,
    proj,
    outs,
    comb,
    lse_out,
    lse_in,
    wout,
    part,
    sib,
    fwd,
    xin,
    wb_ref,
    wc_ref,
    wx_ref,
    wq_ref,
    wk_ref,
    wv_ref,
    send_sem,
    tok_sem,
    main_sem,
    kv_sem,
    out_sem,
    sum_sem,
    local_sem,
):
    g = lax.axis_index("grp")
    s = lax.axis_index("sp")
    t = lax.axis_index("tp")
    across = {"grp": 1 - g}
    sibling = t + 1 - 2 * lax.rem(t, 2)
    far = lax.rem(t + 2, n_tp)
    far_sibling = lax.rem(sibling + 2, n_tp)
    depth = wb_hbm.shape[0]
    half = depth // 2
    rows_own, width = tokens_ref.shape
    count = rows_own * n_tp
    total = count * n_sp
    sub = rows_own // 2
    ch = wb_hbm.shape[1] // n_sp

    def block(index, size):
        return pl.ds(pl.multiple_of(index * size, size), size)

    local = []
    for d in range(n_sp):
        for k, ref in ((0, oconv_ref), (1, oattn_ref)):
            local.append(
                pltpu.make_async_copy(
                    ref.at[pl.ds(d * ch, ch)],
                    wout.at[pl.ds((2 * d + k) * ch, ch)],
                    local_sem.at[2 * d + k],
                )
            )
    weights_in = [
        pltpu.make_async_copy(src, dst, local_sem.at[2 * n_sp + k])
        for k, (src, dst) in enumerate(
            (
                (wb_hbm, wb_ref),
                (wc_hbm, wc_ref),
                (wx_hbm, wx_ref),
                (wq_hbm, wq_ref),
                (wk_hbm, wk_ref),
                (wv_hbm, wv_ref),
            )
        )
    ]
    for copy in weights_in + local:
        copy.start()

    barrier = pltpu.get_barrier_semaphore()
    for by in range(1, n_sp):
        pl.semaphore_signal(
            barrier, inc=1, device_id={"sp": lax.rem(s + by, n_sp)}, device_id_type=MESH
        )
    for by in range(1, n_tp):
        pl.semaphore_signal(
            barrier, inc=1, device_id={"tp": lax.rem(t + by, n_tp)}, device_id_type=MESH
        )
    pl.semaphore_signal(barrier, inc=1, device_id=across, device_id_type=MESH)
    pl.semaphore_wait(barrier, n_sp + n_tp - 1)

    used = [0]
    sent = []

    def send(src, dst, arrival, device, when=None):
        index = used[0]
        used[0] += 1
        copy = pltpu.make_async_remote_copy(
            src_ref=src,
            dst_ref=dst,
            send_sem=send_sem.at[index],
            recv_sem=arrival,
            device_id=device,
            device_id_type=MESH,
        )
        sent.append((copy, when))
        if when is None:
            copy.start()
        else:
            pl.when(when)(copy.start)
        return copy

    def arrived(ref, arrival):
        pltpu.make_async_remote_copy(
            src_ref=ref,
            dst_ref=ref,
            send_sem=send_sem.at[0],
            recv_sem=arrival,
            device_id=across,
            device_id_type=MESH,
        ).wait_recv()

    def both(a, b):
        return b if a is None else jnp.logical_and(a, b)

    def tok_block(z, x):
        return tok.at[block(z * n_tp + x, rows_own)]

    def tok_spread(src, z, step, when):
        arrival = tok_sem.at[z * n_tp + t]
        dst = tok_block(z, t)
        if step >= 0:
            send(src, dst, arrival, {"sp": lax.rem(s + 1, n_sp)}, both(when, s < n_sp - 1))
        if step <= 0:
            send(src, dst, arrival, {"sp": lax.rem(s + n_sp - 1, n_sp)}, both(when, s > 0))
        send(src, dst, arrival, {"tp": far}, when)
        send(src, dst, arrival, {"tp": sibling}, when)

    def tok_round(h):
        for step in (1, -1):
            z = lax.rem(s - step * h + n_sp, n_sp)
            exists = (s >= h) if step > 0 else (s + h < n_sp)

            @pl.when(exists)
            def _(z=z):
                arrived(tok_block(z, t), tok_sem.at[z * n_tp + t])

            tok_spread(tok_block(z, t), z, step, exists)

    def tok_far(z, when=None):
        arrival = tok_sem.at[z * n_tp + far]

        @pl.when(True if when is None else when)
        def _():
            arrived(tok_block(z, far), arrival)

        send(tok_block(z, far), tok_block(z, far), arrival, {"tp": sibling}, when)

    def far_round(h):
        for step in (1, -1):
            exists = (s >= h) if step > 0 else (s + h < n_sp)
            tok_far(lax.rem(s - step * h + n_sp, n_sp), exists)

    def main_rows(z, g_half):
        return wmain.at[block(2 * z + g_half, half)]

    def kv_rows(z, g_half):
        return wkv.at[block(2 * z + g_half, half)]

    def weights_out(h):
        for step in (1, -1):
            exists = (s + h < n_sp) if step > 0 else (s >= h)
            d = lax.rem(s + step * h + n_sp, n_sp)
            to = {"sp": d}
            send(kv_rows(s, g), kv_rows(s, g), kv_sem.at[s], to, exists)
            send(packed.at[d, block(g, half)], main_rows(s, g), main_sem.at[s], to, exists)

    def weights_over(h):
        for step in (1, -1):
            exists = (s >= h) if step > 0 else (s + h < n_sp)
            z = lax.rem(s - step * h + n_sp, n_sp)
            for rows, sems in ((kv_rows, kv_sem), (main_rows, main_sem)):

                @pl.when(exists)
                def _(rows=rows, sems=sems, z=z):
                    arrived(rows(z, g), sems.at[z])

                send(rows(z, g), rows(z, g), sems.at[n_sp + z], across, exists)

    tok_spread(tokens_ref, s, 0, None)
    tok[block(s * n_tp + t, rows_own), :] = tokens_ref[...]
    for copy in weights_in:
        copy.wait()
    for d in range(n_sp):
        cols = slice(d * ch, (d + 1) * ch)
        packed[d, :, : 2 * ch] = jnp.concatenate([wb_ref[:, cols], wc_ref[:, cols]], axis=1)
        packed[d, :, 2 * ch :] = jnp.concatenate([wx_ref[:, cols], wq_ref[:, cols]], axis=1)
    stacked = jnp.concatenate([wk_ref[...], wv_ref[...]], axis=0).astype(F32)
    wkv[block(s, depth), :] = stacked.T.astype(BF16)
    wmain[block(s, depth), :] = packed[s]

    tok_round(1)
    for h in range(1, n_sp):
        weights_out(h)
    tok_far(s)
    for h in range(2, n_sp):
        tok_round(h)
        far_round(h - 1)
        weights_over(h - 1)
    weights_over(n_sp - 1)
    far_round(n_sp - 1)
    for by in range(n_sp):
        z = lax.rem(s + by, n_sp)
        arrived(tok_block(z, sibling), tok_sem.at[z * n_tp + sibling])
        arrived(tok_block(z, far_sibling), tok_sem.at[z * n_tp + far_sibling])

    def normalize(i, unused):
        rows = block(i, rows_own)
        xf = tok[rows, :].astype(F32)
        square = jnp.sum(xf * xf, axis=-1, keepdims=True)
        normed[rows, :] = (xf * gain_ref[...]).astype(BF16)
        scale = lax.rsqrt(square / width + 1e-05)
        proj[rows, :] = jnp.broadcast_to(scale, (rows_own, proj.shape[1]))
        return unused

    lax.fori_loop(0, n_sp * n_tp, normalize, 0)
    scale_rows = proj[:, :1]
    gate_row = gate_ref[pl.ds(s, 1), :]
    gate_column = jnp.broadcast_to(gate_row, (LANES, total)).T[:, :1]
    taps = taps_ref.shape[0]
    taps_own = jnp.zeros((taps, ch), F32)
    for d in range(n_sp):
        taps_own = jnp.where(s == d, taps_ref[:, d * ch : (d + 1) * ch], taps_own)

    for by in range(1, n_sp):
        z = lax.rem(s + by, n_sp)
        arrived(main_rows(z, 1 - g), main_sem.at[n_sp + z])
        arrived(kv_rows(z, 1 - g), kv_sem.at[n_sp + z])

    def project(weight):
        return (
            jnp.dot(normed[...], weight, preferred_element_type=F32) * scale_rows
        ).astype(BF16)

    main = project(wmain[...])
    kv = project(wkv[...])
    gate_b = main[:, :ch].astype(F32)
    conv_src = main[:, ch : 2 * ch].astype(F32) * main[:, 2 * ch : 3 * ch].astype(F32)
    conv_src = conv_src.astype(BF16).astype(F32)
    filtered = jnp.zeros((total, ch), F32)
    for tap in range(taps):
        back = taps - 1 - tap
        moved = conv_src
        if back:
            moved = jnp.concatenate([jnp.zeros((back, ch), F32), conv_src[: total - back]], axis=0)
        filtered = filtered + taps_own[tap : tap + 1] * moved
    conv_out = (gate_b * filtered).astype(BF16)
    query = main[:, 3 * ch :] * BF16(HD**-0.5)
    keys, values = kv[:, :HD], kv[:, HD:]
    for d in reversed(range(n_sp)):
        rows = slice(d * count, (d + 1) * count)
        seen = (d + 1) * count
        score = lax.dot_general(
            query[rows],
            keys[:seen],
            (((1,), (1,)), ((), ())),
            preferred_element_type=F32,
        )
        score = score + gate_column[rows] - gate_row[:, :seen]
        q_pos = d * count + lax.broadcasted_iota(jnp.int32, (count, seen), 0)
        visible = lax.broadcasted_iota(jnp.int32, (count, seen), 1) <= q_pos
        score = jnp.where(visible, score, -1e30)
        row_max = jnp.max(score, axis=-1, keepdims=True)
        weight = jnp.exp(score - row_max)
        row_sum = jnp.sum(weight, axis=-1, keepdims=True)
        out = jnp.dot(weight.astype(BF16), values[:seen], preferred_element_type=F32)
        attn_out = (out / row_sum).astype(BF16)
        both_out = jnp.concatenate([conv_out[rows], attn_out], axis=1)
        for r in range(2):
            for k in range(n_tp):
                start = k * rows_own + r * sub
                outs[r, d, k * sub : (k + 1) * sub] = both_out[start : start + sub]
        logs = jnp.broadcast_to(row_max + jnp.log(row_sum), (count, LANES)).T
        lse_out[d] = logs[: lse_out.shape[1]]
        other = s != d
        send(outs.at[0, d], comb.at[0, s], out_sem.at[s], {"sp": d}, other)
    for d in range(n_sp):
        other = s != d
        send(outs.at[1, d], comb.at[1, s], out_sem.at[n_sp + s], {"sp": d}, other)
        send(lse_out.at[d], lse_in.at[s], out_sem.at[2 * n_sp + s], {"sp": d}, other)
    for r in range(2):
        comb[r, s] = outs[r, s]
    lse_in[s] = lse_out[s]
    for copy in local:
        copy.wait()

    chunks = 2
    wide = width // chunks

    def relay(r, c):
        cols = pl.ds(c * wide, wide)
        base = 3 * (chunks * r + c)
        for k in range(2):
            arrived(sib.at[r, k, :, cols], sum_sem.at[base + k])
        pair = part[r, far, :, cols].astype(F32) + sib[r, 1, :, cols].astype(F32)
        fwd[r, :, cols] = pair.astype(BF16)
        send(fwd.at[r, :, cols], xin.at[r, :, cols], sum_sem.at[base + 2], {"tp": far})

    last = None
    for r in range(2):
        for by in range(1, n_sp):
            z = lax.rem(s + by, n_sp)
            arrived(comb.at[r, z], out_sem.at[r * n_sp + z])
        gathered = jnp.concatenate([comb[r, d] for d in range(n_sp)], axis=1)
        for c in range(chunks):
            cols = pl.ds(c * wide, wide)
            term = jnp.dot(gathered, wout[:, cols], preferred_element_type=F32).astype(BF16)
            for k in range(n_tp):
                part[r, k, :, cols] = term[k * sub : (k + 1) * sub]
            for k, owner in ((1, far_sibling), (0, sibling)):
                send(
                    part.at[r, owner, :, cols],
                    sib.at[r, k, :, cols],
                    sum_sem.at[3 * (chunks * r + c) + k],
                    {"tp": sibling},
                )
            if last is not None:
                relay(*last)
            last = (r, c)
    relay(*last)
    for by in range(1, n_sp):
        z = lax.rem(s + by, n_sp)
        arrived(lse_in.at[z], out_sem.at[2 * n_sp + z])
    for d in range(n_sp):
        lse_ref[d : d + 1, :] = lse_in[d, :1]
    for r in range(2):
        for c in range(chunks):
            cols = pl.ds(c * wide, wide)
            arrived(xin.at[r, :, cols], sum_sem.at[3 * (chunks * r + c) + 2])
            whole = part[r, t, :, cols].astype(F32) + sib[r, 0, :, cols].astype(F32)
            whole = whole + xin[r, :, cols].astype(F32)
            mixed_ref[r * sub : (r + 1) * sub, cols] = whole.astype(BF16)
    for copy, when in sent:
        if when is None:
            copy.wait_send()
        else:
            pl.when(when)(copy.wait_send)


COPIES = 128


def in_one_kernel(
    n_sp,
    n_tp,
    tokens,
    norm_gain,
    conv_b_w,
    conv_c_w,
    conv_x_w,
    query_w,
    key_w,
    value_w,
    conv_taps,
    gate_cache,
    out_conv_w,
    out_attn_w,
):
    rows, width = tokens.shape
    count = rows * n_tp
    depth, channels = conv_b_w.shape
    heads = gate_cache.shape[1]
    kv_width = key_w.shape[1] + value_w.shape[1]
    total = gate_cache.shape[0]
    main_width = (3 * channels + query_w.shape[1]) // n_sp
    pair_width = (channels + query_w.shape[1]) // n_sp
    vmem = pl.BlockSpec(memory_space=pltpu.VMEM)
    hbm = pl.BlockSpec(memory_space=pl.ANY)
    out_rows = out_conv_w.shape[0] + out_attn_w.shape[0]
    dma = pltpu.SemaphoreType.DMA
    mixed, log_rows = pl.pallas_call(
        functools.partial(layer_kernel, n_sp, n_tp),
        out_shape=(
            jax.ShapeDtypeStruct((rows, width), BF16),
            jax.ShapeDtypeStruct((heads, count), F32),
        ),
        in_specs=[vmem] * 2 + [hbm] * 6 + [vmem] * 2 + [hbm] * 2,
        out_specs=(vmem, vmem),
        scratch_shapes=[
            pltpu.VMEM((total, width), BF16),
            pltpu.VMEM((total, width), BF16),
            pltpu.VMEM((n_sp, depth, main_width), BF16),
            pltpu.VMEM((width, main_width), BF16),
            pltpu.VMEM((width, kv_width), BF16),
            pltpu.VMEM((total, LANES), F32),
            pltpu.VMEM((2, n_sp, count // 2, pair_width), BF16),
            pltpu.VMEM((2, n_sp, count // 2, pair_width), BF16),
            pltpu.VMEM((n_sp, 8, count), F32),
            pltpu.VMEM((n_sp, 8, count), F32),
            pltpu.VMEM((out_rows, width), BF16),
            pltpu.VMEM((2, n_tp, rows // 2, width), BF16),
            pltpu.VMEM((2, 2, rows // 2, width), BF16),
            pltpu.VMEM((2, rows // 2, width), BF16),
            pltpu.VMEM((2, rows // 2, width), BF16),
            pltpu.VMEM(conv_b_w.shape, BF16),
            pltpu.VMEM(conv_c_w.shape, BF16),
            pltpu.VMEM(conv_x_w.shape, BF16),
            pltpu.VMEM(query_w.shape, BF16),
            pltpu.VMEM(key_w.shape[::-1], BF16),
            pltpu.VMEM(value_w.shape[::-1], BF16),
            dma((COPIES,)),
            dma((n_sp * n_tp,)),
            dma((2 * n_sp,)),
            dma((2 * n_sp,)),
            dma((3 * n_sp,)),
            dma((12,)),
            dma((2 * n_sp + 6,)),
        ],
        compiler_params=pltpu.CompilerParams(
            collective_id=0, has_side_effects=True, vmem_limit_bytes=60 * 1024 * 1024
        ),
    )(
        tokens,
        norm_gain.reshape(1, width),
        conv_b_w,
        conv_c_w,
        conv_x_w,
        query_w,
        key_w.T,
        value_w.T,
        conv_taps,
        gate_cache.T,
        out_conv_w,
        out_attn_w,
    )
    return mixed, log_rows.T


def passed_along(value, axis, by):
    count = lax.axis_size(axis)
    pairs = [(i, i + by) for i in range(count) if 0 <= i + by < count]
    return lax.ppermute(value, axis, pairs)


def on_device(
    tokens,
    norm_gain,
    conv_b_w,
    conv_c_w,
    conv_x_w,
    query_w,
    key_w,
    value_w,
    conv_taps,
    gate_cache,
    out_conv_w,
    out_attn_w,
):
    rows = lax.all_gather(tokens, "tp", axis=0, tiled=True)
    count = rows.shape[0]
    xf = rows.astype(jnp.float32)
    scale_rows = lax.rsqrt(jnp.mean(xf * xf, axis=-1, keepdims=True) + 1e-05)
    normed = (xf * norm_gain).astype(jnp.bfloat16)

    def contract_all(pieces):
        width = pieces[0].shape[0]
        return tuple(
            (jnp.dot(normed, piece, preferred_element_type=jnp.float32) for piece in pieces)
        )

    conv_sums = contract_all(
        (
            lax.all_gather(conv_b_w, "sp", axis=0, tiled=True),
            lax.all_gather(conv_c_w, "sp", axis=0, tiled=True),
            lax.all_gather(conv_x_w, "sp", axis=0, tiled=True),
        )
    )
    attn_sums = contract_all(
        (
            lax.all_gather(query_w, "sp", axis=0, tiled=True),
            lax.all_gather(key_w, "sp", axis=0, tiled=True),
            lax.all_gather(value_w, "sp", axis=0, tiled=True),
        )
    )
    sums = conv_sums + attn_sums
    gate_b, gate_c, conv_in, query, key, value = [
        (total * scale_rows).astype(jnp.bfloat16) for total in sums
    ]
    taps = conv_taps.shape[0]
    channels = conv_in.shape[1]
    conv_src = (gate_c.astype(jnp.float32) * conv_in.astype(jnp.float32)).astype(jnp.bfloat16)
    earlier = passed_along(conv_src[count - (taps - 1) :], "sp", 1)
    padded = jnp.concatenate([earlier, conv_src], axis=0)
    filtered = jnp.zeros((count, channels), jnp.float32)
    for tap in range(taps):
        filtered = filtered + conv_taps[tap][None, :] * padded[tap : tap + count].astype(
            jnp.float32
        )
    conv_out = (gate_b.astype(jnp.float32) * filtered).astype(jnp.bfloat16)
    heads_dev = gate_cache.shape[1]
    kv_dev = key.shape[1] // HD
    group = heads_dev // kv_dev
    half = count // 2
    sp_index = lax.axis_index("sp")
    own_start = sp_index * count
    scale = HD ** (-0.5)
    later_query = query[half:]
    later_start = own_start + half

    def prepare(q_rows, begin):
        heads_q = q_rows.reshape(half, kv_dev, group, HD)
        q_gate = lax.dynamic_slice_in_dim(gate_cache, begin, half, 0).T.reshape(
            kv_dev, group, half, 1
        )
        q_pos = begin + jnp.arange(half, dtype=jnp.int32)
        return (heads_q, q_gate, q_pos)

    sides = (prepare(query[:half], own_start), prepare(later_query, later_start))

    def absorb(carry, side, key_rows, value_rows, begin):
        heads_q, q_gate, q_pos = side
        run_max, run_sum, acc = carry
        width = key_rows.shape[0]
        key_heads = key_rows.reshape(width, kv_dev, HD)
        value_heads = value_rows.reshape(width, kv_dev, HD)
        score = (
            jnp.einsum("qgjd,kgd->gjqk", heads_q, key_heads, preferred_element_type=jnp.float32)
            * scale
        )
        key_gate = lax.dynamic_slice_in_dim(gate_cache, begin, width, 0).T.reshape(
            kv_dev, group, 1, width
        )
        score = score + q_gate - key_gate
        mask = (begin + jnp.arange(width, dtype=jnp.int32))[None, :] <= q_pos[:, None]
        score = jnp.where(mask, score, -1e30)
        new_max = jnp.maximum(run_max, jnp.max(score, axis=-1))
        weight = jnp.where(mask, jnp.exp(score - new_max[..., None]), 0.0)
        factor = jnp.exp(run_max - new_max)
        new_sum = run_sum * factor + jnp.sum(weight, axis=-1)
        product = jnp.einsum(
            "gjqk,kgd->gjqd",
            weight.astype(jnp.bfloat16),
            value_heads,
            preferred_element_type=jnp.float32,
        )
        return (new_max, new_sum, acc * factor[..., None] + product)

    def guarded(carry, side, key_rows, value_rows, begin):

        def visit_rows(state):
            return absorb(state, side, key_rows, value_rows, begin)

        def keep(state):
            return state

        return lax.cond(begin <= side[2][half - 1], visit_rows, keep, carry)

    def absorb_both(carry, key_rows, value_rows, begin):
        return (
            guarded(carry[0], sides[0], key_rows, value_rows, begin),
            guarded(carry[1], sides[1], key_rows, value_rows, begin),
        )

    def fresh():
        return (
            jnp.full((kv_dev, group, half), -1e30, jnp.float32),
            jnp.zeros((kv_dev, group, half), jnp.float32),
            jnp.zeros((kv_dev, group, half, HD), jnp.float32),
        )

    key_rows = lax.all_gather(key, "sp", axis=0, tiled=True)
    value_rows = lax.all_gather(value, "sp", axis=0, tiled=True)
    width = key_rows.shape[0]
    step = 512
    key_blocks = key_rows.reshape(width // step, step, key_rows.shape[1])
    value_blocks = value_rows.reshape(width // step, step, value_rows.shape[1])
    firsts = step * jnp.arange(width // step, dtype=jnp.int32)

    def visit(state, inputs):
        return (absorb_both(state, inputs[0], inputs[1], inputs[2]), None)

    result, unused = lax.scan(visit, (fresh(), fresh()), (key_blocks, value_blocks, firsts))

    def finish(state):
        run_max, run_sum, acc = state
        out = (
            (acc / run_sum[..., None])
            .transpose(2, 0, 1, 3)
            .reshape(half, heads_dev * HD)
            .astype(jnp.bfloat16)
        )
        lse = (run_max + jnp.log(run_sum)).transpose(2, 0, 1).reshape(half, heads_dev)
        return (out, lse)

    early_out, early_lse = finish(result[0])
    later_out, later_lse = finish(result[1])
    attn_out = jnp.concatenate([early_out, later_out], axis=0)
    log_total = jnp.concatenate([early_lse, later_lse], axis=0)
    term = jnp.dot(conv_out, out_conv_w, preferred_element_type=jnp.float32)
    mixed = lax.psum_scatter(
        (term + jnp.dot(attn_out, out_attn_w, preferred_element_type=jnp.float32)).astype(
            jnp.bfloat16
        ),
        "tp",
        scatter_dimension=0,
        tiled=True,
    )
    return (mixed, log_total)


def solution(mesh):
    placed = (
        P(("grp", "sp", "tp"), None),
        P(),
        P("sp", "tp"),
        P("sp", "tp"),
        P("sp", "tp"),
        P("sp", "tp"),
        P("sp", "tp"),
        P("sp", "tp"),
        P(None, "tp"),
        P("grp", "tp"),
        P("tp", None),
        P("tp", None),
    )
    sizes = dict(mesh.shape)

    def on_one(*args):
        channels, key_width = args[2].shape[1], args[6].shape[1]
        grid = (sizes["grp"], sizes["sp"], sizes["tp"])
        fits = channels == sizes["sp"] * HD and key_width == HD
        if grid == (2, 4, 4) and fits and args[9].shape[1] == sizes["sp"]:
            return in_one_kernel(sizes["sp"], sizes["tp"], *args)
        return on_device(*args)

    return jax.shard_map(
        on_one,
        mesh=mesh,
        in_specs=placed,
        out_specs=(P(("grp", "sp", "tp"), None), P(("grp", "sp"), "tp")),
        check_vma=False,
    )
```

```python
import functools

import jax
import jax.numpy as jnp
from jax import lax
from jax.experimental import pallas as pl
from jax.experimental.pallas import tpu as pltpu
from jax.sharding import PartitionSpec as P

HD = 64
LANES = 128
MESH = pl.DeviceIdType.MESH
F32 = jnp.float32
BF16 = jnp.bfloat16


def layer_kernel(
    n_sp,
    n_tp,
    tokens_ref,
    gain_ref,
    wb_hbm,
    wc_hbm,
    wx_hbm,
    wq_hbm,
    wk_hbm,
    wv_hbm,
    taps_ref,
    gate_ref,
    oconv_ref,
    oattn_ref,
    mixed_ref,
    lse_ref,
    tok,
    normed,
    packed,
    wmain,
    wkv,
    proj,
    outs,
    comb,
    lse_out,
    lse_in,
    wout,
    part,
    sib,
    fwd,
    xin,
    wb_ref,
    wc_ref,
    wx_ref,
    wq_ref,
    wk_ref,
    wv_ref,
    send_sem,
    tok_sem,
    main_sem,
    kv_sem,
    out_sem,
    sum_sem,
    local_sem,
):
    g = lax.axis_index("grp")
    s = lax.axis_index("sp")
    t = lax.axis_index("tp")
    across = {"grp": 1 - g}
    sibling = t + 1 - 2 * lax.rem(t, 2)
    far = lax.rem(t + 2, n_tp)
    far_sibling = lax.rem(sibling + 2, n_tp)
    depth = wb_hbm.shape[0]
    half = depth // 2
    rows_own, width = tokens_ref.shape
    count = rows_own * n_tp
    total = count * n_sp
    sub = rows_own // 2
    ch = wb_hbm.shape[1] // n_sp

    def block(index, size):
        return pl.ds(pl.multiple_of(index * size, size), size)

    local = []
    for d in range(n_sp):
        for k, ref in ((0, oconv_ref), (1, oattn_ref)):
            local.append(
                pltpu.make_async_copy(
                    ref.at[pl.ds(d * ch, ch)],
                    wout.at[pl.ds((2 * d + k) * ch, ch)],
                    local_sem.at[2 * d + k],
                )
            )
    weights_in = [
        pltpu.make_async_copy(src, dst, local_sem.at[2 * n_sp + k])
        for k, (src, dst) in enumerate(
            (
                (wb_hbm, wb_ref),
                (wc_hbm, wc_ref),
                (wx_hbm, wx_ref),
                (wq_hbm, wq_ref),
                (wk_hbm, wk_ref),
                (wv_hbm, wv_ref),
            )
        )
    ]
    for copy in weights_in + local:
        copy.start()

    barrier = pltpu.get_barrier_semaphore()
    for by in range(1, n_sp):
        pl.semaphore_signal(
            barrier, inc=1, device_id={"sp": lax.rem(s + by, n_sp)}, device_id_type=MESH
        )
    for by in range(1, n_tp):
        pl.semaphore_signal(
            barrier, inc=1, device_id={"tp": lax.rem(t + by, n_tp)}, device_id_type=MESH
        )
    pl.semaphore_signal(barrier, inc=1, device_id=across, device_id_type=MESH)
    pl.semaphore_wait(barrier, n_sp + n_tp - 1)

    used = [0]
    sent = []

    def send(src, dst, arrival, device, when=None):
        index = used[0]
        used[0] += 1
        copy = pltpu.make_async_remote_copy(
            src_ref=src,
            dst_ref=dst,
            send_sem=send_sem.at[index],
            recv_sem=arrival,
            device_id=device,
            device_id_type=MESH,
        )
        sent.append((copy, when))
        if when is None:
            copy.start()
        else:
            pl.when(when)(copy.start)
        return copy

    def arrived(ref, arrival):
        pltpu.make_async_remote_copy(
            src_ref=ref,
            dst_ref=ref,
            send_sem=send_sem.at[0],
            recv_sem=arrival,
            device_id=across,
            device_id_type=MESH,
        ).wait_recv()

    def both(a, b):
        return b if a is None else jnp.logical_and(a, b)

    def tok_block(z, x, p):
        return tok.at[block((z * n_tp + x) * 2 + p, sub)]

    def tok_arrival(z, x, p):
        return tok_sem.at[(z * n_tp + x) * 2 + p]

    def tok_spread(src, z, p, step, when):
        arrival = tok_arrival(z, t, p)
        dst = tok_block(z, t, p)
        if step >= 0:
            send(src, dst, arrival, {"sp": lax.rem(s + 1, n_sp)}, both(when, s < n_sp - 1))
        if step <= 0:
            send(src, dst, arrival, {"sp": lax.rem(s + n_sp - 1, n_sp)}, both(when, s > 0))
        send(src, dst, arrival, {"tp": far}, when)
        send(src, dst, arrival, {"tp": sibling}, when)

    def tok_round(h):
        for p in range(2):
            for step in (1, -1):
                z = lax.rem(s - step * h + n_sp, n_sp)
                exists = (s >= h) if step > 0 else (s + h < n_sp)

                @pl.when(exists)
                def _(z=z):
                    arrived(tok_block(z, t, p), tok_arrival(z, t, p))

                tok_spread(tok_block(z, t, p), z, p, step, exists)

    def tok_far(z, when=None):
        for p in range(2):
            arrival = tok_arrival(z, far, p)
            here = tok_block(z, far, p)

            @pl.when(True if when is None else when)
            def _():
                arrived(here, arrival)

            send(here, here, arrival, {"tp": sibling}, when)

    def far_round(h):
        for step in (1, -1):
            exists = (s >= h) if step > 0 else (s + h < n_sp)
            tok_far(lax.rem(s - step * h + n_sp, n_sp), exists)

    def main_rows(z, g_half):
        return wmain.at[block(2 * z + g_half, half)]

    def kv_rows(z, g_half):
        return wkv.at[block(2 * z + g_half, half)]

    def weights_out(h):
        for step in (1, -1):
            exists = (s + h < n_sp) if step > 0 else (s >= h)
            d = lax.rem(s + step * h + n_sp, n_sp)
            to = {"sp": d}
            send(kv_rows(s, g), kv_rows(s, g), kv_sem.at[s], to, exists)
            send(packed.at[d, block(g, half)], main_rows(s, g), main_sem.at[s], to, exists)

    def weights_over(h):
        for step in (1, -1):
            exists = (s >= h) if step > 0 else (s + h < n_sp)
            z = lax.rem(s - step * h + n_sp, n_sp)
            for rows, sems in ((kv_rows, kv_sem), (main_rows, main_sem)):

                @pl.when(exists)
                def _(rows=rows, sems=sems, z=z):
                    arrived(rows(z, g), sems.at[z])

                send(rows(z, g), rows(z, g), sems.at[n_sp + z], across, exists)

    for p in range(2):
        tok_spread(tokens_ref.at[pl.ds(p * sub, sub)], s, p, 0, None)
    tok[block(s * n_tp + t, rows_own), :] = tokens_ref[...]
    for copy in weights_in:
        copy.wait()
    for d in range(n_sp):
        cols = slice(d * ch, (d + 1) * ch)
        packed[d, :, : 2 * ch] = jnp.concatenate([wb_ref[:, cols], wc_ref[:, cols]], axis=1)
        packed[d, :, 2 * ch :] = jnp.concatenate([wx_ref[:, cols], wq_ref[:, cols]], axis=1)
    stacked = jnp.concatenate([wk_ref[...], wv_ref[...]], axis=0).astype(F32)
    wkv[block(s, depth), :] = stacked.T.astype(BF16)
    wmain[block(s, depth), :] = packed[s]

    tok_round(1)
    for h in range(1, n_sp):
        weights_out(h)
    tok_far(s)
    for h in range(2, n_sp):
        tok_round(h)
        far_round(h - 1)
        weights_over(h - 1)
    weights_over(n_sp - 1)
    far_round(n_sp - 1)
    for by in range(n_sp):
        z = lax.rem(s + by, n_sp)
        for p in range(2):
            for x in (sibling, far_sibling):
                arrived(tok_block(z, x, p), tok_arrival(z, x, p))

    def normalize(i, unused):
        rows = block(i, rows_own)
        xf = tok[rows, :].astype(F32)
        square = jnp.sum(xf * xf, axis=-1, keepdims=True)
        normed[rows, :] = (xf * gain_ref[...]).astype(BF16)
        scale = lax.rsqrt(square / width + 1e-05)
        proj[rows, :] = jnp.broadcast_to(scale, (rows_own, proj.shape[1]))
        return unused

    lax.fori_loop(0, n_sp * n_tp, normalize, 0)
    scale_rows = proj[:, :1]
    gate_row = gate_ref[pl.ds(s, 1), :]
    gate_column = jnp.broadcast_to(gate_row, (LANES, total)).T[:, :1]
    taps = taps_ref.shape[0]
    taps_own = jnp.zeros((taps, ch), F32)
    for d in range(n_sp):
        taps_own = jnp.where(s == d, taps_ref[:, d * ch : (d + 1) * ch], taps_own)

    for by in range(1, n_sp):
        z = lax.rem(s + by, n_sp)
        arrived(main_rows(z, 1 - g), main_sem.at[n_sp + z])
        arrived(kv_rows(z, 1 - g), kv_sem.at[n_sp + z])

    def project(weight):
        return (
            jnp.dot(normed[...], weight, preferred_element_type=F32) * scale_rows
        ).astype(BF16)

    main = project(wmain[...])
    kv = project(wkv[...])
    gate_b = main[:, :ch].astype(F32)
    conv_src = main[:, ch : 2 * ch].astype(F32) * main[:, 2 * ch : 3 * ch].astype(F32)
    conv_src = conv_src.astype(BF16).astype(F32)
    filtered = jnp.zeros((total, ch), F32)
    for tap in range(taps):
        back = taps - 1 - tap
        moved = conv_src
        if back:
            moved = jnp.concatenate([jnp.zeros((back, ch), F32), conv_src[: total - back]], axis=0)
        filtered = filtered + taps_own[tap : tap + 1] * moved
    conv_out = (gate_b * filtered).astype(BF16)
    query = main[:, 3 * ch :] * BF16(HD**-0.5)
    keys, values = kv[:, :HD], kv[:, HD:]
    for d in reversed(range(n_sp)):
        rows = slice(d * count, (d + 1) * count)
        seen = (d + 1) * count
        score = lax.dot_general(
            query[rows],
            keys[:seen],
            (((1,), (1,)), ((), ())),
            preferred_element_type=F32,
        )
        score = score + gate_column[rows] - gate_row[:, :seen]
        q_pos = d * count + lax.broadcasted_iota(jnp.int32, (count, seen), 0)
        visible = lax.broadcasted_iota(jnp.int32, (count, seen), 1) <= q_pos
        score = jnp.where(visible, score, -1e30)
        row_max = jnp.max(score, axis=-1, keepdims=True)
        weight = jnp.exp(score - row_max)
        row_sum = jnp.sum(weight, axis=-1, keepdims=True)
        out = jnp.dot(weight.astype(BF16), values[:seen], preferred_element_type=F32)
        attn_out = (out / row_sum).astype(BF16)
        both_out = jnp.concatenate([conv_out[rows], attn_out], axis=1)
        for r in range(2):
            for k in range(n_tp):
                start = k * rows_own + r * sub
                outs[r, d, k * sub : (k + 1) * sub] = both_out[start : start + sub]
        logs = jnp.broadcast_to(row_max + jnp.log(row_sum), (count, LANES)).T
        lse_out[d] = logs[: lse_out.shape[1]]
        other = s != d
        send(outs.at[0, d], comb.at[0, s], out_sem.at[s], {"sp": d}, other)
    for d in range(n_sp):
        other = s != d
        send(outs.at[1, d], comb.at[1, s], out_sem.at[n_sp + s], {"sp": d}, other)
        send(lse_out.at[d], lse_in.at[s], out_sem.at[2 * n_sp + s], {"sp": d}, other)
    for r in range(2):
        comb[r, s] = outs[r, s]
    lse_in[s] = lse_out[s]
    for copy in local:
        copy.wait()

    chunks = 2
    wide = width // chunks

    def relay(r, c):
        cols = pl.ds(c * wide, wide)
        base = 3 * (chunks * r + c)
        for k in range(2):
            arrived(sib.at[r, k, :, cols], sum_sem.at[base + k])
        pair = part[r, far, :, cols].astype(F32) + sib[r, 1, :, cols].astype(F32)
        fwd[r, :, cols] = pair.astype(BF16)
        send(fwd.at[r, :, cols], xin.at[r, :, cols], sum_sem.at[base + 2], {"tp": far})

    last = None
    for r in range(2):
        for by in range(1, n_sp):
            z = lax.rem(s + by, n_sp)
            arrived(comb.at[r, z], out_sem.at[r * n_sp + z])
        gathered = jnp.concatenate([comb[r, d] for d in range(n_sp)], axis=1)
        for c in range(chunks):
            cols = pl.ds(c * wide, wide)
            term = jnp.dot(gathered, wout[:, cols], preferred_element_type=F32).astype(BF16)
            for k in range(n_tp):
                part[r, k, :, cols] = term[k * sub : (k + 1) * sub]
            for k, owner in ((1, far_sibling), (0, sibling)):
                send(
                    part.at[r, owner, :, cols],
                    sib.at[r, k, :, cols],
                    sum_sem.at[3 * (chunks * r + c) + k],
                    {"tp": sibling},
                )
            if last is not None:
                relay(*last)
            last = (r, c)
    relay(*last)
    for by in range(1, n_sp):
        z = lax.rem(s + by, n_sp)
        arrived(lse_in.at[z], out_sem.at[2 * n_sp + z])
    for d in range(n_sp):
        lse_ref[d : d + 1, :] = lse_in[d, :1]
    for r in range(2):
        for c in range(chunks):
            cols = pl.ds(c * wide, wide)
            arrived(xin.at[r, :, cols], sum_sem.at[3 * (chunks * r + c) + 2])
            whole = part[r, t, :, cols].astype(F32) + sib[r, 0, :, cols].astype(F32)
            whole = whole + xin[r, :, cols].astype(F32)
            mixed_ref[r * sub : (r + 1) * sub, cols] = whole.astype(BF16)
    for copy, when in sent:
        if when is None:
            copy.wait_send()
        else:
            pl.when(when)(copy.wait_send)


COPIES = 192


def in_one_kernel(
    n_sp,
    n_tp,
    tokens,
    norm_gain,
    conv_b_w,
    conv_c_w,
    conv_x_w,
    query_w,
    key_w,
    value_w,
    conv_taps,
    gate_cache,
    out_conv_w,
    out_attn_w,
):
    rows, width = tokens.shape
    count = rows * n_tp
    depth, channels = conv_b_w.shape
    heads = gate_cache.shape[1]
    kv_width = key_w.shape[1] + value_w.shape[1]
    total = gate_cache.shape[0]
    main_width = (3 * channels + query_w.shape[1]) // n_sp
    pair_width = (channels + query_w.shape[1]) // n_sp
    vmem = pl.BlockSpec(memory_space=pltpu.VMEM)
    hbm = pl.BlockSpec(memory_space=pl.ANY)
    out_rows = out_conv_w.shape[0] + out_attn_w.shape[0]
    dma = pltpu.SemaphoreType.DMA
    mixed, log_rows = pl.pallas_call(
        functools.partial(layer_kernel, n_sp, n_tp),
        out_shape=(
            jax.ShapeDtypeStruct((rows, width), BF16),
            jax.ShapeDtypeStruct((heads, count), F32),
        ),
        in_specs=[vmem] * 2 + [hbm] * 6 + [vmem] * 2 + [hbm] * 2,
        out_specs=(vmem, vmem),
        scratch_shapes=[
            pltpu.VMEM((total, width), BF16),
            pltpu.VMEM((total, width), BF16),
            pltpu.VMEM((n_sp, depth, main_width), BF16),
            pltpu.VMEM((width, main_width), BF16),
            pltpu.VMEM((width, kv_width), BF16),
            pltpu.VMEM((total, LANES), F32),
            pltpu.VMEM((2, n_sp, count // 2, pair_width), BF16),
            pltpu.VMEM((2, n_sp, count // 2, pair_width), BF16),
            pltpu.VMEM((n_sp, 8, count), F32),
            pltpu.VMEM((n_sp, 8, count), F32),
            pltpu.VMEM((out_rows, width), BF16),
            pltpu.VMEM((2, n_tp, rows // 2, width), BF16),
            pltpu.VMEM((2, 2, rows // 2, width), BF16),
            pltpu.VMEM((2, rows // 2, width), BF16),
            pltpu.VMEM((2, rows // 2, width), BF16),
            pltpu.VMEM(conv_b_w.shape, BF16),
            pltpu.VMEM(conv_c_w.shape, BF16),
            pltpu.VMEM(conv_x_w.shape, BF16),
            pltpu.VMEM(query_w.shape, BF16),
            pltpu.VMEM(key_w.shape[::-1], BF16),
            pltpu.VMEM(value_w.shape[::-1], BF16),
            dma((COPIES,)),
            dma((2 * n_sp * n_tp,)),
            dma((2 * n_sp,)),
            dma((2 * n_sp,)),
            dma((3 * n_sp,)),
            dma((12,)),
            dma((2 * n_sp + 6,)),
        ],
        compiler_params=pltpu.CompilerParams(
            collective_id=0, has_side_effects=True, vmem_limit_bytes=60 * 1024 * 1024
        ),
    )(
        tokens,
        norm_gain.reshape(1, width),
        conv_b_w,
        conv_c_w,
        conv_x_w,
        query_w,
        key_w.T,
        value_w.T,
        conv_taps,
        gate_cache.T,
        out_conv_w,
        out_attn_w,
    )
    return mixed, log_rows.T


def passed_along(value, axis, by):
    count = lax.axis_size(axis)
    pairs = [(i, i + by) for i in range(count) if 0 <= i + by < count]
    return lax.ppermute(value, axis, pairs)


def on_device(
    tokens,
    norm_gain,
    conv_b_w,
    conv_c_w,
    conv_x_w,
    query_w,
    key_w,
    value_w,
    conv_taps,
    gate_cache,
    out_conv_w,
    out_attn_w,
):
    rows = lax.all_gather(tokens, "tp", axis=0, tiled=True)
    count = rows.shape[0]
    xf = rows.astype(jnp.float32)
    scale_rows = lax.rsqrt(jnp.mean(xf * xf, axis=-1, keepdims=True) + 1e-05)
    normed = (xf * norm_gain).astype(jnp.bfloat16)

    def contract_all(pieces):
        width = pieces[0].shape[0]
        return tuple(
            (jnp.dot(normed, piece, preferred_element_type=jnp.float32) for piece in pieces)
        )

    conv_sums = contract_all(
        (
            lax.all_gather(conv_b_w, "sp", axis=0, tiled=True),
            lax.all_gather(conv_c_w, "sp", axis=0, tiled=True),
            lax.all_gather(conv_x_w, "sp", axis=0, tiled=True),
        )
    )
    attn_sums = contract_all(
        (
            lax.all_gather(query_w, "sp", axis=0, tiled=True),
            lax.all_gather(key_w, "sp", axis=0, tiled=True),
            lax.all_gather(value_w, "sp", axis=0, tiled=True),
        )
    )
    sums = conv_sums + attn_sums
    gate_b, gate_c, conv_in, query, key, value = [
        (total * scale_rows).astype(jnp.bfloat16) for total in sums
    ]
    taps = conv_taps.shape[0]
    channels = conv_in.shape[1]
    conv_src = (gate_c.astype(jnp.float32) * conv_in.astype(jnp.float32)).astype(jnp.bfloat16)
    earlier = passed_along(conv_src[count - (taps - 1) :], "sp", 1)
    padded = jnp.concatenate([earlier, conv_src], axis=0)
    filtered = jnp.zeros((count, channels), jnp.float32)
    for tap in range(taps):
        filtered = filtered + conv_taps[tap][None, :] * padded[tap : tap + count].astype(
            jnp.float32
        )
    conv_out = (gate_b.astype(jnp.float32) * filtered).astype(jnp.bfloat16)
    heads_dev = gate_cache.shape[1]
    kv_dev = key.shape[1] // HD
    group = heads_dev // kv_dev
    half = count // 2
    sp_index = lax.axis_index("sp")
    own_start = sp_index * count
    scale = HD ** (-0.5)
    later_query = query[half:]
    later_start = own_start + half

    def prepare(q_rows, begin):
        heads_q = q_rows.reshape(half, kv_dev, group, HD)
        q_gate = lax.dynamic_slice_in_dim(gate_cache, begin, half, 0).T.reshape(
            kv_dev, group, half, 1
        )
        q_pos = begin + jnp.arange(half, dtype=jnp.int32)
        return (heads_q, q_gate, q_pos)

    sides = (prepare(query[:half], own_start), prepare(later_query, later_start))

    def absorb(carry, side, key_rows, value_rows, begin):
        heads_q, q_gate, q_pos = side
        run_max, run_sum, acc = carry
        width = key_rows.shape[0]
        key_heads = key_rows.reshape(width, kv_dev, HD)
        value_heads = value_rows.reshape(width, kv_dev, HD)
        score = (
            jnp.einsum("qgjd,kgd->gjqk", heads_q, key_heads, preferred_element_type=jnp.float32)
            * scale
        )
        key_gate = lax.dynamic_slice_in_dim(gate_cache, begin, width, 0).T.reshape(
            kv_dev, group, 1, width
        )
        score = score + q_gate - key_gate
        mask = (begin + jnp.arange(width, dtype=jnp.int32))[None, :] <= q_pos[:, None]
        score = jnp.where(mask, score, -1e30)
        new_max = jnp.maximum(run_max, jnp.max(score, axis=-1))
        weight = jnp.where(mask, jnp.exp(score - new_max[..., None]), 0.0)
        factor = jnp.exp(run_max - new_max)
        new_sum = run_sum * factor + jnp.sum(weight, axis=-1)
        product = jnp.einsum(
            "gjqk,kgd->gjqd",
            weight.astype(jnp.bfloat16),
            value_heads,
            preferred_element_type=jnp.float32,
        )
        return (new_max, new_sum, acc * factor[..., None] + product)

    def guarded(carry, side, key_rows, value_rows, begin):

        def visit_rows(state):
            return absorb(state, side, key_rows, value_rows, begin)

        def keep(state):
            return state

        return lax.cond(begin <= side[2][half - 1], visit_rows, keep, carry)

    def absorb_both(carry, key_rows, value_rows, begin):
        return (
            guarded(carry[0], sides[0], key_rows, value_rows, begin),
            guarded(carry[1], sides[1], key_rows, value_rows, begin),
        )

    def fresh():
        return (
            jnp.full((kv_dev, group, half), -1e30, jnp.float32),
            jnp.zeros((kv_dev, group, half), jnp.float32),
            jnp.zeros((kv_dev, group, half, HD), jnp.float32),
        )

    key_rows = lax.all_gather(key, "sp", axis=0, tiled=True)
    value_rows = lax.all_gather(value, "sp", axis=0, tiled=True)
    width = key_rows.shape[0]
    step = 512
    key_blocks = key_rows.reshape(width // step, step, key_rows.shape[1])
    value_blocks = value_rows.reshape(width // step, step, value_rows.shape[1])
    firsts = step * jnp.arange(width // step, dtype=jnp.int32)

    def visit(state, inputs):
        return (absorb_both(state, inputs[0], inputs[1], inputs[2]), None)

    result, unused = lax.scan(visit, (fresh(), fresh()), (key_blocks, value_blocks, firsts))

    def finish(state):
        run_max, run_sum, acc = state
        out = (
            (acc / run_sum[..., None])
            .transpose(2, 0, 1, 3)
            .reshape(half, heads_dev * HD)
            .astype(jnp.bfloat16)
        )
        lse = (run_max + jnp.log(run_sum)).transpose(2, 0, 1).reshape(half, heads_dev)
        return (out, lse)

    early_out, early_lse = finish(result[0])
    later_out, later_lse = finish(result[1])
    attn_out = jnp.concatenate([early_out, later_out], axis=0)
    log_total = jnp.concatenate([early_lse, later_lse], axis=0)
    term = jnp.dot(conv_out, out_conv_w, preferred_element_type=jnp.float32)
    mixed = lax.psum_scatter(
        (term + jnp.dot(attn_out, out_attn_w, preferred_element_type=jnp.float32)).astype(
            jnp.bfloat16
        ),
        "tp",
        scatter_dimension=0,
        tiled=True,
    )
    return (mixed, log_total)


def solution(mesh):
    placed = (
        P(("grp", "sp", "tp"), None),
        P(),
        P("sp", "tp"),
        P("sp", "tp"),
        P("sp", "tp"),
        P("sp", "tp"),
        P("sp", "tp"),
        P("sp", "tp"),
        P(None, "tp"),
        P("grp", "tp"),
        P("tp", None),
        P("tp", None),
    )
    sizes = dict(mesh.shape)

    def on_one(*args):
        channels, key_width = args[2].shape[1], args[6].shape[1]
        grid = (sizes["grp"], sizes["sp"], sizes["tp"])
        fits = channels == sizes["sp"] * HD and key_width == HD
        if grid == (2, 4, 4) and fits and args[9].shape[1] == sizes["sp"]:
            return in_one_kernel(sizes["sp"], sizes["tp"], *args)
        return on_device(*args)

    return jax.shard_map(
        on_one,
        mesh=mesh,
        in_specs=placed,
        out_specs=(P(("grp", "sp", "tp"), None), P(("grp", "sp"), "tp")),
        check_vma=False,
    )
```
